512 devices in a mesh: ep: 32 (over z, core), tp: 16 (over y, x).
Axes of the slice: x: 4, y: 4, z: 16, core: 2. Of those that a mesh axis runs over, the one named last changes fastest.
Arguments:
- queries: bfloat16 [8192, 4096], P('ep', 'tp'), may hold values from -6 to 6
- keys: bfloat16 [8192, 1024], P('ep', 'tp'), may hold values from -6 to 6
- values: bfloat16 [8192, 1024], P('ep', 'tp'), may hold values from -6 to 6
- query_gain: float32 [64], replicated, may hold values from 1 to 11
- key_gain: float32 [64], replicated, may hold values from 1 to 11
- moe_rows: bfloat16 [8192, 4096], P('ep', 'tp'), may hold values from -14 to 14
- route_ids: int32 [8192, 2], P('ep'), may hold values from 0 to 31, all different within a row; in each aligned block of 256 rows (0 to 255, 256 to 511, ...) at most 24 rows name the same one
- group_weight: float32 [8192], P('ep'), may hold values from 0.2 to 1
- expert_weight: float32 [8192, 2], P('ep'), may hold values from 0.05 to 1
- expert_gate: bfloat16 [32, 4096, 2048], P('ep', None, 'tp'), may hold values from -0.09375 to 0.09375
- expert_up: bfloat16 [32, 4096, 2048], P('ep', None, 'tp'), may hold values from -0.09375 to 0.09375
- expert_down: bfloat16 [32, 2048, 4096], P('ep', None, 'tp'), may hold values from -0.125 to 0.125
Outputs:
- attended: bfloat16 [8192, 4096], P('ep', 'tp')
- moe_out: bfloat16 [8192, 4096], P('ep', 'tp')
The draws below stay inside these ranges and needn't reach their ends.
Inputs may be any that keep to these rules, and one draw needn't show every extreme that they name: `route_ids`: each row names 2 different experts. Among the rows of one device no expert is named by more than 24 rows, and in every draw some expert is named by exactly 24 of them.
All inputs are finite; a program needn't handle non-finite values.
Results may differ from the reference program's by a relative error of at most 0.0055.
The reference program's roundings to bfloat16 on the way count: a program that leaves them out, or rounds other values in their place, can miss the bound.
Values may be sent and summed in bfloat16 or wider, within the bound.
No kernel may reach another device: no remote copies, remote signals or barrier semaphores. Data moves between devices by JAX's collectives and lax.ppermute only.
A program may use at most 128 MiB of HBM per device.

```python
import math
import jax
import jax.numpy as jnp
import numpy as np
from jax import lax

D = 4096
HEAD_DIM = 64
HEADS = 64
KV_HEADS = 16
FF = 2048
GRID_W = 64
TOPK = 2
TOK_DEV = 256
TOKENS = 8192
EXPERTS = 32
CAP = 24
N_EP = 32


def query_key_pair(key):
    folded = jax.random.fold_in(key, 17)
    key_one, key_two = jax.random.split(folded, 2)
    query_draw = jnp.clip(jax.random.normal(key_one, (TOKENS, HEADS * HEAD_DIM), jnp.float32), -6.0, 6.0)
    key_draw = jnp.clip(jax.random.normal(key_two, (TOKENS, KV_HEADS * HEAD_DIM), jnp.float32), -6.0, 6.0)
    return (query_draw, key_draw)


def draw_queries(key, part):
    return query_key_pair(key)[0].astype(jnp.bfloat16)


def draw_keys(key, part):
    return query_key_pair(key)[1].astype(jnp.bfloat16)


def gain_draw(key, salt):
    folded = jax.random.fold_in(key, salt)
    spread = 1.5 * jnp.exp(jax.random.uniform(folded, (HEAD_DIM,), jnp.float32, -0.3, 0.3))
    return spread


def draw_query_gain(key, part):
    return gain_draw(key, 31)


def draw_key_gain(key, part):
    return gain_draw(key, 37)


def draw_moe_rows(key, part):
    folded = jax.random.fold_in(key, 23)
    key_one, key_two = jax.random.split(folded)
    base_part = jnp.clip(jax.random.normal(key_one, (TOKENS, D), jnp.float32), -4.0, 4.0)
    scales = jnp.exp(jax.random.uniform(key_two, (TOKENS, 1), jnp.float32, -1.2, 1.2))
    return (base_part * scales).astype(jnp.bfloat16)


def steps_of(rng, extent, cuts, least, top_value):
    factor_of = 1.0
    for dim, parts in cuts:
        heights = jax.random.uniform(jax.random.fold_in(jax.random.fold_in(rng, 6), dim), (parts,), jnp.float32, least / len(cuts), top_value / len(cuts))
        factor_of = factor_of * jnp.repeat(jnp.exp(heights), extent[dim] // parts).reshape((-1,) + (1,) * (len(extent) - 1 - dim))
    return factor_of


def assign_block(stream_key, own, number, rows, count, top, bound, slope):
    sequence = jax.random.permutation(stream_key, count)
    crowded, ordinary = load_shares(count, rows * top, bound, slope, True), load_shares(count, rows * top, bound, slope, False)
    places = jnp.arange(count)

    def named(lengths, offset_by):
        used = int((lengths > 0).sum())
        fixed = max(1, used // 4)
        moved = fixed + (places - fixed + offset_by * (used - fixed)) % max(1, count - fixed)
        return jnp.zeros((count,), jnp.int32).at[sequence[jnp.where(places < fixed, places, moved)]].set(jnp.asarray(lengths, jnp.int32))

    lengths = jnp.where(number % 4 == 0, named(crowded, number // 4), named(ordinary, number - number // 4 - 1))
    mixed = jax.random.permutation(jax.random.fold_in(own, 3), count)
    source_of, taker = mixed[0:count // 2 * 2:2], mixed[1:count // 2 * 2:2]
    margin = jnp.minimum(lengths[source_of] - 1, bound - lengths[taker]) // 2
    margin = jnp.where((source_of == sequence[0]) | (taker == sequence[0]) | (lengths[taker] == 0), 0, jnp.maximum(margin, 0))
    moved = jax.random.randint(jax.random.fold_in(own, 4), (count // 2,), 0, 1 << 20) % (margin + 1)
    lengths = lengths.at[source_of].add(-moved).at[taker].add(moved)
    labels = jnp.searchsorted(jnp.cumsum(lengths), jnp.arange(rows * top), side="right").astype(jnp.int32)
    table = labels.reshape(top, rows).T
    table = table[jax.random.permutation(jax.random.fold_in(own, 1), rows)]
    offset_by = jax.random.randint(jax.random.fold_in(own, 2), (rows, 1), 0, top)
    return jnp.take_along_axis(table, (jnp.arange(top)[None, :] + offset_by) % top, axis=1)


def load_shares(amount, total, bound, skew, full):
    portions = [(1 << 20) // math.isqrt(grade ** skew) + 1 for grade in range(1, amount + 1)]
    largest = bound if full else min(bound, max(-(-total // amount), total * portions[0] // sum(portions)))
    least = 1 if total - largest >= amount - 1 else 0
    counts, spare = [largest] + [least] * (amount - 1), total - largest - least * (amount - 1)
    while spare > 0:
        candidates = [i for i in range(1, amount) if counts[i] < largest] or [i for i in range(1, amount) if counts[i] < bound]
        whole, remaining = sum([portions[i] for i in candidates]), spare
        for i in candidates:
            addition = min(bound - counts[i], max(1, remaining * portions[i] // whole), spare)
            counts[i] = counts[i] + addition
            spare = spare - addition
    return np.array(counts)


def normal_values(own_key, dims, deviation, bound, cuts=(), kind=jnp.bfloat16):
    entries = deviation * jax.random.normal(own_key, dims, jnp.float32)
    if cuts:
        entries = entries * steps_of(own_key, dims, cuts, -0.22, 0.18)
    return jnp.clip(entries, -bound, bound).astype(kind)


def setup_inputs(seed: int = 0) -> dict:
    key_of = jax.random.split(jax.random.key(seed), 13)
    queries = draw_queries(jax.random.fold_in(key_of[12], 71), 0)
    keys = draw_keys(jax.random.fold_in(key_of[12], 71), 0)
    values = normal_values(key_of[2], (TOKENS, KV_HEADS * HEAD_DIM), 1.0, 6.0, ((0, 32), (1, 16)))
    query_gain = draw_query_gain(jax.random.fold_in(key_of[12], 71), 0)
    key_gain = draw_key_gain(jax.random.fold_in(key_of[12], 71), 0)
    moe_rows = draw_moe_rows(jax.random.fold_in(key_of[12], 71), 0)
    route_ids_keys = jax.random.split(jax.random.fold_in(key_of[6], 1), TOKENS // TOK_DEV)
    route_ids_turns = jax.random.permutation(jax.random.fold_in(key_of[6], 3), TOKENS // TOK_DEV)
    route_ids = jax.vmap(lambda own, number: assign_block(jax.random.fold_in(key_of[6], 2), own, number, TOK_DEV, EXPERTS, TOPK, CAP, 1))(route_ids_keys, route_ids_turns).reshape((TOKENS, TOPK))
    group_weight = jnp.clip(jnp.exp(math.log(1.0) - 1.609438 * jax.random.uniform(key_of[7], (TOKENS,), jnp.float32) ** steps_of(key_of[7], (TOKENS,), ((0, 32),), -0.2, 0.2)), 0.2, 1.0)
    expert_weight = jnp.clip(jnp.exp(math.log(1.0) - 2.9957323 * jax.random.uniform(key_of[8], (TOKENS, TOPK), jnp.float32) ** steps_of(key_of[8], (TOKENS, TOPK), ((0, 32),), -0.2, 0.2)), 0.05, 1.0)
    expert_gate = normal_values(key_of[9], (EXPERTS, D, FF), D ** -0.5, 0.09375, ((0, 32), (2, 16)))
    expert_up = normal_values(key_of[10], (EXPERTS, D, FF), D ** -0.5, 0.09375, ((0, 32), (2, 16)))
    expert_down = normal_values(key_of[11], (EXPERTS, FF, D), FF ** -0.5, 0.125, ((0, 32), (2, 16)))
    return dict(queries=queries, keys=keys, values=values, query_gain=query_gain, key_gain=key_gain, moe_rows=moe_rows, route_ids=route_ids, group_weight=group_weight, expert_weight=expert_weight, expert_gate=expert_gate, expert_up=expert_up, expert_down=expert_down)


def rotary_tables(position):
    pair_count = HEAD_DIM // 4
    grid_pos = jnp.stack([position // GRID_W, position % GRID_W], axis=-1).astype(jnp.float32)
    frequency = 10000.0 ** (-jnp.arange(pair_count, dtype=jnp.float32) / pair_count)
    angles = grid_pos[:, :, None] * frequency
    return (jnp.cos(angles), jnp.sin(angles))

def normed_rotated(rows_in, gain, cosine, sine_of):
    row_count, head_count = (rows_in.shape[0], rows_in.shape[1])
    pair_count = HEAD_DIM // 4
    scaled = rows_in * lax.rsqrt(lax.optimization_barrier(jnp.mean(rows_in * rows_in, axis=-1, keepdims=True)) + 1e-06) * gain
    parted = scaled.reshape(row_count, head_count, 2, 2, pair_count)
    first_half, second = (parted[:, :, :, 0, :], parted[:, :, :, 1, :])
    cos_b, sin_b = (cosine[:, None], sine_of[:, None])
    turned = jnp.stack([first_half * cos_b - second * sin_b, second * cos_b + first_half * sin_b], axis=3)
    return turned.reshape(row_count, head_count, HEAD_DIM).astype(jnp.bfloat16)

def attend_reference(queries, keys, values, query_gain, key_gain):
    group_size = HEADS // KV_HEADS
    cosine, sine_of = rotary_tables(jnp.arange(TOKENS, dtype=jnp.int32))
    query_rot = normed_rotated(queries.astype(jnp.float32).reshape(TOKENS, HEADS, HEAD_DIM), query_gain, cosine, sine_of)
    key_rot = normed_rotated(keys.astype(jnp.float32).reshape(TOKENS, KV_HEADS, HEAD_DIM), key_gain, cosine, sine_of)
    value_heads = values.reshape(TOKENS, KV_HEADS, HEAD_DIM)
    block_rows = math.gcd(TOKENS, 512)
    query_heads = query_rot.reshape(TOKENS // block_rows, block_rows, KV_HEADS, group_size, HEAD_DIM).transpose(2, 0, 1, 3, 4)

    def one_head(inputs):
        q_part, k_head, v_head = inputs

        def one_block(q_blk):
            scores = jnp.einsum('qgd,sd->gqs', q_blk.astype(jnp.float32), k_head.astype(jnp.float32)) * HEAD_DIM ** (-0.5)
            weights = jnp.exp(scores - lax.optimization_barrier(jnp.max(scores, axis=-1, keepdims=True)))
            denominator = lax.optimization_barrier(jnp.sum(weights, axis=-1))
            low_weights = lax.optimization_barrier(weights.astype(jnp.bfloat16)).astype(jnp.float32)
            mixed_out = jnp.einsum('gqs,sd->qgd', low_weights, v_head.astype(jnp.float32))
            return (mixed_out / denominator.T[:, :, None]).astype(jnp.bfloat16)
        return lax.map(one_block, q_part)
    output = lax.map(one_head, (query_heads, key_rot.transpose(1, 0, 2), value_heads.transpose(1, 0, 2)))
    return output.transpose(1, 2, 0, 3, 4).reshape(TOKENS, HEADS * HEAD_DIM)

def experts_reference(moe_rows, route_ids, group_weight, expert_weight, expert_gate, expert_up, expert_down):
    picks = TOK_DEV * TOPK
    route_list = route_ids.reshape(N_EP, picks)
    one_hot = (route_list[:, :, None] == jnp.arange(EXPERTS, dtype=jnp.int32)[None, None, :]).astype(jnp.int32)
    rank_of = lax.optimization_barrier(jnp.sum((jnp.cumsum(one_hot, axis=1) - one_hot) * one_hot, axis=-1))
    source = jnp.arange(N_EP, dtype=jnp.int32)[:, None]
    slot_of = route_list * (N_EP * CAP) + source * CAP + rank_of
    owner_of = source * TOK_DEV + jnp.arange(picks, dtype=jnp.int32)[None, :] // TOPK
    slot_owner = jnp.full((EXPERTS * N_EP * CAP,), TOKENS, jnp.int32).at[slot_of.reshape(-1)].set(owner_of.reshape(-1))
    padded = jnp.concatenate([moe_rows, jnp.zeros((1, D), moe_rows.dtype)], axis=0)
    routed = padded[slot_owner].reshape(EXPERTS, N_EP * CAP, D)

    def one_expert(inputs):
        rows_in, w_gate, w_up, w_down = inputs
        widened = rows_in.astype(jnp.float32)
        inv_rms = lax.rsqrt(lax.optimization_barrier(jnp.mean(widened * widened, axis=-1, keepdims=True)) + 1e-06)
        gate_act = jnp.dot(rows_in, w_gate, preferred_element_type=jnp.float32) * inv_rms
        up_act = jnp.dot(rows_in, w_up, preferred_element_type=jnp.float32) * inv_rms
        hidden = (jax.nn.silu(gate_act) * up_act).astype(jnp.bfloat16)
        return jnp.dot(hidden, w_down, preferred_element_type=jnp.float32).astype(jnp.bfloat16)
    results = lax.map(one_expert, (routed, expert_gate, expert_up, expert_down)).reshape(EXPERTS * N_EP * CAP, D)
    picked = results[slot_of.reshape(TOKENS, TOPK)].astype(jnp.float32)
    mixing = group_weight[:, None] * expert_weight / lax.optimization_barrier(jnp.sum(expert_weight, axis=-1, keepdims=True))
    return lax.optimization_barrier(jnp.sum(mixing[:, :, None] * picked, axis=1)).astype(jnp.bfloat16)

def reference(queries, keys, values, query_gain, key_gain, moe_rows, route_ids, group_weight, expert_weight, expert_gate, expert_up, expert_down):
    attended = attend_reference(queries, keys, values, query_gain, key_gain)
    moe_out = experts_reference(moe_rows, route_ids, group_weight, expert_weight, expert_gate, expert_up, expert_down)
    return (attended, moe_out)
```

```python
import functools

import jax
import jax.numpy as jnp
from jax import lax
from jax.experimental import pallas as pl
from jax.experimental.pallas import tpu as pltpu
from jax.sharding import Mesh
from jax.sharding import PartitionSpec as P

D = 4096
HEAD_DIM = 64
GRID_W = 64
TOK = 256
EXPERTS = 32
CAP = 24
SLOTS = EXPERTS * CAP
HALF = SLOTS // 2
PAIRS = HEAD_DIM // 4
EXTRA = 8
EP = ("z", "c")
TP = ("y", "x")
CX = ("c", "x")
BF = jnp.bfloat16
F32 = jnp.float32


def iota(shape, dim):
    return lax.broadcasted_iota(jnp.int32, shape, dim)


def mm(a, b):
    return jnp.dot(a, b, preferred_element_type=F32)


def column(row):
    n = row.shape[1]
    eye = iota((n, n), 0) == iota((n, n), 1)
    return jnp.sum(jnp.where(eye, jnp.broadcast_to(row, (n, n)), 0.0), axis=1, keepdims=True)


def slots_of(ids):
    e = iota((EXPERTS, TOK), 0)
    hits = [e == ids[k : k + 1] for k in range(2)]
    member = jnp.where(hits[0] | hits[1], 1.0, 0.0).astype(BF)
    before = jnp.where(iota((TOK, TOK), 0) < iota((TOK, TOK), 1), 1.0, 0.0).astype(BF)
    rank = mm(member, before)
    return [
        ids[k : k + 1] * CAP
        + jnp.sum(jnp.where(hits[k], rank, 0.0), axis=0, keepdims=True).astype(jnp.int32)
        for k in range(2)
    ]


def route_fn(ids, rows):
    first, second = slots_of(ids)
    s = iota((SLOTS, TOK), 0)
    chosen = jnp.where((s == first) | (s == second), 1.0, 0.0).astype(BF)
    return mm(chosen, rows).astype(BF)


def combine_fn(ids, group_weight, expert_weight, results):
    total = expert_weight[0:1] + expert_weight[1:2]
    out = None
    for k, slot in enumerate(slots_of(ids)):
        mix = column(group_weight * expert_weight[k : k + 1] / total)
        at = column(slot.astype(F32)).astype(jnp.int32)
        chosen = jnp.where(iota((TOK, SLOTS), 1) == at, 1.0, 0.0).astype(BF)
        part = mix * mm(chosen, results)
        out = part if out is None else out + part
    return out.astype(BF)


def rotated(x, gain, table):
    mean = jnp.sum(x * x, axis=0, keepdims=True) * (1.0 / HEAD_DIM)
    scaled = x * lax.rsqrt(mean + 1e-06) * gain
    parts = []
    for axis in range(2):
        lo = 2 * PAIRS * axis
        x1, x2 = scaled[lo : lo + PAIRS], scaled[lo + PAIRS : lo + 2 * PAIRS]
        cosine = table[PAIRS * axis : PAIRS * (axis + 1)]
        sine = table[PAIRS * (axis + 2) : PAIRS * (axis + 3)]
        parts += [x1 * cosine - x2 * sine, x2 * cosine + x1 * sine]
    return jnp.concatenate(parts, axis=0)


def rope_fn(queries, keys_t, values_t, table):
    q_t = queries.astype(F32).T
    q_gain, k_gain = table[64:128], table[128:192]
    heads = []
    for h in range(4):
        turned = rotated(q_t[h * HEAD_DIM : (h + 1) * HEAD_DIM], q_gain, table) * 0.125
        heads.append(jnp.concatenate([turned, jnp.zeros_like(turned)], axis=0).T.astype(BF))
    k = rotated(keys_t.astype(F32), k_gain, table)
    kv = jnp.concatenate([k, values_t.astype(F32)], axis=0).T.astype(BF)
    return heads, kv


def gate_up_fn(get_tokens, get_weight, put):
    ones = jnp.ones((EXTRA, 256), BF)
    rows = []
    sums = []
    for c in range(2):
        blocks = [get_tokens(4 * c + x) for x in range(4)]
        square = None
        for b in blocks:
            w = b.astype(F32)
            square = w * w if square is None else square + w * w
        total = None
        for _ in range(3):
            piece = square.astype(BF)
            square = square - piece.astype(F32)
            part = lax.dot_general(ones, piece, (((1,), (1,)), ((), ())), preferred_element_type=F32)
            total = part if total is None else total + part
        sums.append(total[0:1])
        rows.append(jnp.concatenate(blocks, axis=1))
    sums = jnp.concatenate(sums, axis=1) * 0.125
    high = sums.astype(BF).astype(F32)
    low = (sums - high) * 256.0
    pieces = [v[:, 256 * i : 256 * (i + 1)] for v in (high, low) for i in range(3)]
    extra = jnp.concatenate(pieces + [jnp.zeros((2, 256), F32)], axis=0)
    for s in range(4):
        w = get_weight(s)
        for c in range(2):
            put(s, c * HALF, mm(rows[c], w) * 32.0)
        put(s, SLOTS, extra)


def hidden_fn(get, put):
    sums = get(SLOTS, EXTRA)
    for i in range(3):
        square = (sums[i : i + 1] + sums[i + 3 : i + 4] * (1.0 / 256)) * (8.0 / D)
        inv = lax.rsqrt(column(square) + 1e-06) * (1.0 / 32)
        both = get(256 * i, 256)
        gate, up = both[:, :128] * inv, both[:, 128:] * inv
        put(256 * i, (gate / (1.0 + jnp.exp(-gate)) * up).astype(BF))


def down_fn(get_hidden, get_weight, put):
    rows = [
        [jnp.concatenate([get_hidden(2 * j, c), get_hidden(2 * j + 1, c)], axis=1) for j in range(2)]
        for c in range(2)
    ]
    for s in range(4):
        w = get_weight(s)
        for c in range(2):
            put(c, s, (mm(rows[c][0], w[:256]) + mm(rows[c][1], w[256:])).astype(BF))


def reduce_fn(get):
    return [
        sum(get(4 * c + x).astype(F32) for x in range(4)).astype(BF).reshape(16, CAP, 256)
        for c in range(2)
    ]


def route_kernel(ids, rows, out):
    out[...] = route_fn(ids[...], rows[...])


def combine_kernel(ids, gw, ew, res, out):
    out[...] = combine_fn(ids[...], gw[...], ew[...], res[...])


def rope_kernel(q, k, v, table, q_out, kv_out):
    heads, kv = rope_fn(q[...], k[...], v[...], table[...])
    for h in range(4):
        q_out[h] = heads[h]
    kv_out[...] = kv


def pack_kernel(at, gate, up, down, *outs):
    for s in range(4):
        y, x = lax.rem(at[0] + s, 4), lax.rem(at[1] + s, 4)
        rows = pl.ds(pl.multiple_of(y * 1024, 1024), 1024)
        outs[s][:, 0:128] = gate[rows, :]
        outs[s][:, 128:256] = up[rows, :]
        for i in range(4):
            outs[4 + s][i] = down[i, x]


def gate_up_kernel(at, tokens, w0, w1, w2, w3, out):
    weights = (w0, w1, w2, w3)

    def put(s, row, value):
        out[lax.rem(at[0] + 4 - s, 4), row : row + value.shape[0], :] = value

    gate_up_fn(lambda i: tokens[i], lambda s: weights[s][...], put)


def hidden_kernel(parts, out):
    def put(at, value):
        for y in range(4):
            out[y, at : at + value.shape[0], :] = value

    hidden_fn(lambda at, n: parts[at : at + n, :], put)


def down_kernel(at, hidden, w0, w1, w2, w3, out):
    weights = (w0, w1, w2, w3)

    def put(c, s, value):
        out[c, lax.rem(at[1] + 4 - s, 4)] = value

    down_fn(
        lambda y, c: hidden[y, c * HALF : (c + 1) * HALF, :],
        lambda s: weights[s][...].reshape(512, 256),
        put,
    )


def reduce_kernel(parts, out):
    for c, value in enumerate(reduce_fn(lambda i: parts[i])):
        out[:, c] = value


KEYS = 1024


def attend_kernel(q, kv, out, scores):
    blocks = [(kv, i) for i in range(kv.shape[0] // KEYS)]

    def lanes(v, op):
        parts = [v[:, 128 * i : 128 * (i + 1)] for i in range(v.shape[1] // 128)]
        return functools.reduce(op, parts)

    def score(h, j):
        ref, i = blocks[j]
        s = lax.dot_general(
            q[h], ref[i * KEYS : (i + 1) * KEYS, :], (((1,), (1,)), ((), ())), preferred_element_type=F32
        )
        scores[h, :, j * KEYS : (j + 1) * KEYS] = s
        return lanes(s, jnp.maximum)

    def weigh(h, j, top):
        ref, i = blocks[j]
        p = jnp.exp(scores[h, :, j * KEYS : (j + 1) * KEYS] - top)
        return lanes(p, jnp.add), mm(p.astype(BF), ref[i * KEYS : (i + 1) * KEYS, :])

    n = len(blocks)
    top = functools.reduce(jnp.maximum, [score(0, j) for j in range(n)])
    results = []
    for h in range(2):
        top = jnp.max(top, axis=1, keepdims=True)
        following = total = summed = None
        for j in range(n):
            if h == 0:
                m = score(1, j)
                following = m if following is None else jnp.maximum(following, m)
            t, o = weigh(h, j, top)
            total = t if total is None else total + t
            summed = o if summed is None else summed + o
        top = following
        results.append(summed / jnp.sum(total, axis=1, keepdims=True))
    first = pltpu.roll(results[0], HEAD_DIM, axis=1)
    out[...] = jnp.where(iota(first.shape, 1) < HEAD_DIM, first, results[1]).astype(BF)


def call(kernel, outs, *args, flops=0, scratch=(), vmem=48, space=pltpu.VMEM):
    def spec(a):
        return pl.BlockSpec(memory_space=pltpu.SMEM if a.dtype == jnp.int32 and a.size == 2 else space)

    return pl.pallas_call(
        kernel,
        out_shape=outs,
        in_specs=[spec(a) for a in args],
        out_specs=jax.tree.map(lambda _: pl.BlockSpec(memory_space=space), outs),
        scratch_shapes=scratch,
        cost_estimate=pl.CostEstimate(flops=flops, transcendentals=0, bytes_accessed=0),
        compiler_params=pltpu.CompilerParams(vmem_limit_bytes=vmem << 20),
        name=kernel.__name__,
    )(*args)


def array(*shape, dtype=BF):
    return jax.ShapeDtypeStruct(shape, dtype)


def shifted(blocks, axis):
    return [b if s == 0 else lax.ppermute(b, axis, [(i, (i + s) % 4) for i in range(4)]) for s, b in enumerate(blocks)]


def exchange(a, axes):
    return lax.all_to_all(a, axes, split_axis=0, concat_axis=0, tiled=True)


def rope_table(query_gain, key_gain):
    position = lax.axis_index(EP) * TOK + jnp.arange(TOK, dtype=jnp.int32)
    grid_pos = jnp.stack([position // GRID_W, position % GRID_W], axis=0).astype(F32)
    frequency = 10000.0 ** (-jnp.arange(PAIRS, dtype=F32) / PAIRS)
    angles = (grid_pos[:, None, :] * frequency[None, :, None]).reshape(2 * PAIRS, TOK)
    gains = jnp.concatenate([query_gain, key_gain])
    return jnp.concatenate(
        [jnp.cos(angles), jnp.sin(angles), jnp.broadcast_to(gains[:, None], (2 * HEAD_DIM, TOK))], axis=0
    )


def attend(q, kv):
    scratch = [pltpu.VMEM((2, TOK, kv.shape[0]), F32)]
    return call(attend_kernel, array(TOK, 128), q, kv, flops=2200 << 20, scratch=scratch)


def on_device(
    queries,
    keys,
    values,
    query_gain,
    key_gain,
    moe_rows,
    route_ids,
    group_weight,
    expert_weight,
    expert_gate,
    expert_up,
    expert_down,
):
    tie = lax.optimization_barrier
    ids = route_ids.T
    routed = call(route_kernel, array(SLOTS, 256), ids, moe_rows, flops=4 << 20)
    routed, gate, up, down, queries, keys, values = tie(
        (routed, expert_gate, expert_up, expert_down, queries, keys, values)
    )
    arrived = exchange(routed.reshape(16, 2 * CAP, 256), "z")
    table = rope_table(query_gain, key_gain)
    q_heads, kv = call(
        rope_kernel, (array(4, TOK, 128), array(TOK, 128)), queries, keys.T, values.T, table, flops=4 << 20
    )
    keys_values = lax.all_gather(kv, EP, axis=0, tiled=True)
    at = jnp.stack([lax.axis_index("y"), lax.axis_index("x")]).astype(jnp.int32)
    packed = call(
        pack_kernel,
        (array(1024, 256),) * 4 + (array(4, 128, 256),) * 4,
        at,
        gate[0],
        up[0],
        down[0].reshape(4, 4, 128, 256),
    )
    w_in, w_out = shifted(packed[:4], "y"), shifted(packed[4:], "x")
    arrived, w_in, w_out, q_heads = tie((arrived, w_in, w_out, q_heads))
    sent = arrived.reshape(16, 2, CAP, 256).transpose(1, 0, 2, 3).reshape(2, 1, HALF, 256)
    tokens = exchange(jnp.broadcast_to(sent, (2, 4, HALF, 256)).reshape(8, HALF, 256), CX)
    partial = call(
        gate_up_kernel, array(4, SLOTS + EXTRA, 256, dtype=F32), at, tokens, *w_in, flops=1600 << 20
    )
    products = jnp.sum(exchange(partial.astype(jnp.float16), "y").astype(F32), axis=0)
    hidden = call(hidden_kernel, array(4, SLOTS, 128), products, flops=8 << 20)
    results = call(
        down_kernel, array(2, 4, HALF, 256), at, exchange(hidden, "y"), *w_out, flops=800 << 20
    ).reshape(8, HALF, 256)
    results, q_heads = tie((results, q_heads))
    summands = exchange(results, CX)
    first = attend(q_heads[:2], keys_values)
    summands, first, q_heads = tie((summands, first, q_heads))
    reduced = call(reduce_kernel, array(16, 2, CAP, 256), summands, flops=4 << 20)
    reduced, q_heads = tie((reduced, q_heads))
    returned = exchange(reduced.reshape(16, 2 * CAP, 256), "z")
    second = attend(q_heads[2:], keys_values)
    returned, second = tie((returned, second))
    moe_out = call(
        combine_kernel,
        array(TOK, 256),
        ids,
        group_weight.reshape(1, TOK),
        expert_weight.T,
        returned.reshape(SLOTS, 256),
        flops=8 << 20,
    )
    attended = jnp.concatenate([first, second], axis=1)
    return (attended, moe_out)


def solution(mesh):
    torus = Mesh(mesh.devices.reshape(16, 2, 4, 4), ("z", "c", "y", "x"))
    return jax.shard_map(
        on_device,
        mesh=torus,
        in_specs=(
            P(EP, TP),
            P(EP, TP),
            P(EP, TP),
            P(),
            P(),
            P(EP, TP),
            P(EP, None),
            P(EP),
            P(EP, None),
            P(EP, None, TP),
            P(EP, None, TP),
            P(EP, None, TP),
        ),
        out_specs=(P(EP, TP), P(EP, TP)),
        check_vma=False,
    )
```

```python
import functools

import jax
import jax.numpy as jnp
from jax import lax
from jax.experimental import pallas as pl
from jax.experimental.pallas import tpu as pltpu
from jax.sharding import Mesh
from jax.sharding import PartitionSpec as P

D = 4096
HEAD_DIM = 64
GRID_W = 64
TOK = 256
EXPERTS = 32
CAP = 24
SLOTS = EXPERTS * CAP
HALF = SLOTS // 2
PAIRS = HEAD_DIM // 4
EXTRA = 8
EP = ("z", "c")
TP = ("y", "x")
CX = ("c", "x")
BF = jnp.bfloat16
F32 = jnp.float32


def iota(shape, dim):
    return lax.broadcasted_iota(jnp.int32, shape, dim)


def mm(a, b):
    return jnp.dot(a, b, preferred_element_type=F32)


def column(row):
    n = row.shape[1]
    eye = iota((n, n), 0) == iota((n, n), 1)
    return jnp.sum(jnp.where(eye, jnp.broadcast_to(row, (n, n)), 0.0), axis=1, keepdims=True)


def slots_of(ids):
    e = iota((EXPERTS, TOK), 0)
    hits = [e == ids[k : k + 1] for k in range(2)]
    member = jnp.where(hits[0] | hits[1], 1.0, 0.0).astype(BF)
    before = jnp.where(iota((TOK, TOK), 0) < iota((TOK, TOK), 1), 1.0, 0.0).astype(BF)
    rank = mm(member, before)
    return [
        ids[k : k + 1] * CAP
        + jnp.sum(jnp.where(hits[k], rank, 0.0), axis=0, keepdims=True).astype(jnp.int32)
        for k in range(2)
    ]


def route_fn(ids, rows):
    first, second = slots_of(ids)
    s = iota((SLOTS, TOK), 0)
    chosen = jnp.where((s == first) | (s == second), 1.0, 0.0).astype(BF)
    return mm(chosen, rows).astype(BF)


def combine_fn(ids, group_weight, expert_weight, results):
    total = expert_weight[0:1] + expert_weight[1:2]
    out = None
    for k, slot in enumerate(slots_of(ids)):
        mix = column(group_weight * expert_weight[k : k + 1] / total)
        at = column(slot.astype(F32)).astype(jnp.int32)
        chosen = jnp.where(iota((TOK, SLOTS), 1) == at, 1.0, 0.0).astype(BF)
        part = mix * mm(chosen, results)
        out = part if out is None else out + part
    return out.astype(BF)


def rotated(x, gain, table):
    mean = jnp.sum(x * x, axis=0, keepdims=True) * (1.0 / HEAD_DIM)
    scaled = x * lax.rsqrt(mean + 1e-06) * gain
    parts = []
    for axis in range(2):
        lo = 2 * PAIRS * axis
        x1, x2 = scaled[lo : lo + PAIRS], scaled[lo + PAIRS : lo + 2 * PAIRS]
        cosine = table[PAIRS * axis : PAIRS * (axis + 1)]
        sine = table[PAIRS * (axis + 2) : PAIRS * (axis + 3)]
        parts += [x1 * cosine - x2 * sine, x2 * cosine + x1 * sine]
    return jnp.concatenate(parts, axis=0)


def rope_fn(queries, keys_t, values_t, table):
    q_t = queries.astype(F32).T
    q_gain, k_gain = table[64:128], table[128:192]
    heads = []
    for h in range(4):
        turned = rotated(q_t[h * HEAD_DIM : (h + 1) * HEAD_DIM], q_gain, table) * 0.125
        heads.append(jnp.concatenate([turned, jnp.zeros_like(turned)], axis=0).T.astype(BF))
    k = rotated(keys_t.astype(F32), k_gain, table)
    kv = jnp.concatenate([k, values_t.astype(F32)], axis=0).T.astype(BF)
    return heads, kv


def gate_up_fn(get_tokens, get_weight, put):
    ones = jnp.ones((EXTRA, 256), BF)
    rows = []
    sums = []
    for c in range(2):
        blocks = [get_tokens(4 * c + x) for x in range(4)]
        square = None
        for b in blocks:
            w = b.astype(F32)
            square = w * w if square is None else square + w * w
        total = None
        for _ in range(3):
            piece = square.astype(BF)
            square = square - piece.astype(F32)
            part = lax.dot_general(ones, piece, (((1,), (1,)), ((), ())), preferred_element_type=F32)
            total = part if total is None else total + part
        sums.append(total[0:1])
        rows.append(jnp.concatenate(blocks, axis=1))
    sums = jnp.concatenate(sums, axis=1) * 0.125
    high = sums.astype(BF).astype(F32)
    low = (sums - high) * 256.0
    pieces = [v[:, 256 * i : 256 * (i + 1)] for v in (high, low) for i in range(3)]
    extra = jnp.concatenate(pieces + [jnp.zeros((2, 256), F32)], axis=0)
    for s in range(4):
        w = get_weight(s)
        for c in range(2):
            put(s, c * HALF, mm(rows[c], w) * 32.0)
        put(s, SLOTS, extra)


def hidden_fn(get, put):
    sums = get(SLOTS, EXTRA)
    for i in range(3):
        square = (sums[i : i + 1] + sums[i + 3 : i + 4] * (1.0 / 256)) * (8.0 / D)
        inv = lax.rsqrt(column(square) + 1e-06) * (1.0 / 32)
        both = get(256 * i, 256)
        gate, up = both[:, :128] * inv, both[:, 128:] * inv
        put(256 * i, (gate / (1.0 + jnp.exp(-gate)) * up).astype(BF))


def down_fn(get_hidden, get_weight, put):
    rows = [
        [jnp.concatenate([get_hidden(2 * j, c), get_hidden(2 * j + 1, c)], axis=1) for j in range(2)]
        for c in range(2)
    ]
    for s in range(4):
        w = get_weight(s)
        for c in range(2):
            put(c, s, (mm(rows[c][0], w[:256]) + mm(rows[c][1], w[256:])).astype(BF))


def reduce_fn(get):
    return [
        sum(get(4 * c + x).astype(F32) for x in range(4)).astype(BF).reshape(16, CAP, 256)
        for c in range(2)
    ]


def route_kernel(ids, rows, out):
    out[...] = route_fn(ids[...], rows[...])


def combine_kernel(ids, gw, ew, res, out):
    out[...] = combine_fn(ids[...], gw[...], ew[...], res[...])


def rope_kernel(q, k, v, table, q_first, q_second, kv_first, kv_second):
    heads, kv = rope_fn(q[...], k[...], v[...], table[...])
    for h in range(2):
        q_first[h] = heads[h]
        q_second[h] = heads[2 + h]
    kv_first[...] = kv[: TOK // 2]
    kv_second[...] = kv[TOK // 2 :]


def pack_kernel(at, gate, up, down, *outs):
    for s in range(4):
        y, x = lax.rem(at[0] + s, 4), lax.rem(at[1] + s, 4)
        rows = pl.ds(pl.multiple_of(y * 1024, 1024), 1024)
        outs[s][:, 0:128] = gate[rows, :]
        outs[s][:, 128:256] = up[rows, :]
        for i in range(4):
            outs[4 + s][i] = down[i, x]


def gate_up_kernel(at, tokens, w0, w1, w2, w3, out):
    weights = (w0, w1, w2, w3)

    def put(s, row, value):
        out[lax.rem(at[0] + 4 - s, 4), row : row + value.shape[0], :] = value

    gate_up_fn(lambda i: tokens[i], lambda s: weights[s][...], put)


def hidden_kernel(parts, out):
    def put(at, value):
        for y in range(4):
            out[y, at : at + value.shape[0], :] = value

    hidden_fn(lambda at, n: parts[at : at + n, :], put)


def down_kernel(at, hidden, w0, w1, w2, w3, out):
    weights = (w0, w1, w2, w3)

    def put(c, s, value):
        out[c, lax.rem(at[1] + 4 - s, 4)] = value

    down_fn(
        lambda y, c: hidden[y, c * HALF : (c + 1) * HALF, :],
        lambda s: weights[s][...].reshape(512, 256),
        put,
    )


def reduce_kernel(parts, out):
    for c, value in enumerate(reduce_fn(lambda i: parts[i])):
        out[:, c] = value


KEYS = 1024


def attend_kernel(q, own, other, out, scores):
    blocks = [(ref, i) for ref in (own, other) for i in range(ref.shape[0] // KEYS)]

    def lanes(v, op):
        parts = [v[:, 128 * i : 128 * (i + 1)] for i in range(v.shape[1] // 128)]
        return functools.reduce(op, parts)

    def score(h, j):
        ref, i = blocks[j]
        s = lax.dot_general(
            q[h], ref[i * KEYS : (i + 1) * KEYS, :], (((1,), (1,)), ((), ())), preferred_element_type=F32
        )
        scores[h, :, j * KEYS : (j + 1) * KEYS] = s
        return lanes(s, jnp.maximum)

    def weigh(h, j, top):
        ref, i = blocks[j]
        p = jnp.exp(scores[h, :, j * KEYS : (j + 1) * KEYS] - top)
        return lanes(p, jnp.add), mm(p.astype(BF), ref[i * KEYS : (i + 1) * KEYS, :])

    n = len(blocks)
    top = functools.reduce(jnp.maximum, [score(0, j) for j in range(n)])
    results = []
    for h in range(2):
        top = jnp.max(top, axis=1, keepdims=True)
        following = total = summed = None
        for j in range(n):
            if h == 0:
                m = score(1, j)
                following = m if following is None else jnp.maximum(following, m)
            t, o = weigh(h, j, top)
            total = t if total is None else total + t
            summed = o if summed is None else summed + o
        top = following
        results.append(summed / jnp.sum(total, axis=1, keepdims=True))
    first = pltpu.roll(results[0], HEAD_DIM, axis=1)
    out[...] = jnp.where(iota(first.shape, 1) < HEAD_DIM, first, results[1]).astype(BF)


def call(kernel, outs, *args, flops=0, scratch=(), vmem=20, space=pltpu.VMEM):
    def spec(a):
        return pl.BlockSpec(memory_space=pltpu.SMEM if a.dtype == jnp.int32 and a.size == 2 else space)

    return pl.pallas_call(
        kernel,
        out_shape=outs,
        in_specs=[spec(a) for a in args],
        out_specs=jax.tree.map(lambda _: pl.BlockSpec(memory_space=space), outs),
        scratch_shapes=scratch,
        cost_estimate=pl.CostEstimate(flops=flops, transcendentals=0, bytes_accessed=0),
        compiler_params=pltpu.CompilerParams(vmem_limit_bytes=vmem << 20),
    )(*args)


def array(*shape, dtype=BF):
    return jax.ShapeDtypeStruct(shape, dtype)


def shifted(blocks, axis):
    return [b if s == 0 else lax.ppermute(b, axis, [(i, (i + s) % 4) for i in range(4)]) for s, b in enumerate(blocks)]


def exchange(a, axes):
    return lax.all_to_all(a, axes, split_axis=0, concat_axis=0, tiled=True)


def rope_table(query_gain, key_gain):
    position = lax.axis_index(EP) * TOK + jnp.arange(TOK, dtype=jnp.int32)
    grid_pos = jnp.stack([position // GRID_W, position % GRID_W], axis=0).astype(F32)
    frequency = 10000.0 ** (-jnp.arange(PAIRS, dtype=F32) / PAIRS)
    angles = (grid_pos[:, None, :] * frequency[None, :, None]).reshape(2 * PAIRS, TOK)
    gains = jnp.concatenate([query_gain, key_gain])
    return jnp.concatenate(
        [jnp.cos(angles), jnp.sin(angles), jnp.broadcast_to(gains[:, None], (2 * HEAD_DIM, TOK))], axis=0
    )


def attend(q, own, other):
    scratch = [pltpu.VMEM((2, TOK, 2 * own.shape[0]), F32)]
    return call(attend_kernel, array(TOK, 128), q, own, other, flops=2200 << 20, scratch=scratch, vmem=36)


def doubled(kv, shift):
    moved = [
        lax.ppermute(a, "z", [(i, (i + n) % 16) for i in range(16)])
        for a, n in zip(kv, (shift, -shift))
    ]
    return [jnp.concatenate([a, b], axis=0) for a, b in zip(kv, moved)]


def on_device(
    queries,
    keys,
    values,
    query_gain,
    key_gain,
    moe_rows,
    route_ids,
    group_weight,
    expert_weight,
    expert_gate,
    expert_up,
    expert_down,
):
    tie = lax.optimization_barrier
    ids = route_ids.T
    routed = call(route_kernel, array(SLOTS, 256), ids, moe_rows, flops=4 << 20)
    routed, gate, up, down, queries, keys, values = tie(
        (routed, expert_gate, expert_up, expert_down, queries, keys, values)
    )
    arrived = exchange(routed.reshape(16, 2 * CAP, 256), "z")
    at = jnp.stack([lax.axis_index("y"), lax.axis_index("x")]).astype(jnp.int32)
    packed = call(
        pack_kernel,
        (array(1024, 256),) * 4 + (array(4, 128, 256),) * 4,
        at,
        gate[0],
        up[0],
        down[0].reshape(4, 4, 128, 256),
    )
    w_in = shifted(packed[:4], "y")
    table = rope_table(query_gain, key_gain)
    *q_heads, kv_first, kv_second = call(
        rope_kernel,
        (array(2, TOK, 128),) * 2 + (array(TOK // 2, 128),) * 2,
        queries,
        keys.T,
        values.T,
        table,
        flops=4 << 20,
    )
    kv = [kv_first, kv_second]
    arrived, w_in, w_out, q_heads, kv = tie((arrived, w_in, packed[4:], q_heads, kv))
    sent = arrived.reshape(16, 2, CAP, 256).transpose(1, 0, 2, 3).reshape(2, 1, HALF, 256)
    tokens = exchange(jnp.broadcast_to(sent, (2, 4, HALF, 256)).reshape(8, HALF, 256), CX)
    kv = doubled(doubled(kv, 8), 4)
    tokens, kv = tie((tokens, kv))
    partial = call(
        gate_up_kernel, array(4, SLOTS + EXTRA, 256, dtype=F32), at, tokens, *w_in, flops=1600 << 20
    ).astype(jnp.float16)
    partial, w_out, kv = tie((partial, w_out, kv))
    products = exchange(partial, "y")
    w_out = shifted(w_out, "x")
    kv = doubled(kv, 2)
    products, w_out, kv = tie((products, w_out, kv))
    hidden = call(
        hidden_kernel, array(4, SLOTS, 128), jnp.sum(products.astype(F32), axis=0), flops=8 << 20
    )
    hidden, kv = tie((hidden, kv))
    hidden = exchange(hidden, "y")
    kv = jnp.concatenate(doubled(kv, 1), axis=0)
    hidden, kv = tie((hidden, kv))
    results = call(down_kernel, array(2, 4, HALF, 256), at, hidden, *w_out, flops=800 << 20).reshape(
        8, HALF, 256
    )
    results, kv, q_heads = tie((results, kv, q_heads))
    summands = exchange(results, CX)
    other = lax.ppermute(kv, "c", [(0, 1), (1, 0)])
    attended = jnp.concatenate([attend(q, kv, other) for q in q_heads], axis=1)
    summands, attended = tie((summands, attended))
    reduced = call(reduce_kernel, array(16, 2, CAP, 256), summands, flops=4 << 20)
    returned = exchange(reduced.reshape(16, 2 * CAP, 256), "z")
    moe_out = call(
        combine_kernel,
        array(TOK, 256),
        ids,
        group_weight.reshape(1, TOK),
        expert_weight.T,
        returned.reshape(SLOTS, 256),
        flops=8 << 20,
    )
    return (attended, moe_out)


def solution(mesh):
    torus = Mesh(mesh.devices.reshape(16, 2, 4, 4), ("z", "c", "y", "x"))

    return jax.shard_map(
        on_device,
        mesh=torus,
        in_specs=(
            P(EP, TP),
            P(EP, TP),
            P(EP, TP),
            P(),
            P(),
            P(EP, TP),
            P(EP, None),
            P(EP),
            P(EP, None),
            P(EP, None, TP),
            P(EP, None, TP),
            P(EP, None, TP),
        ),
        out_specs=(P(EP, TP), P(EP, TP)),
        check_vma=False,
    )
```

```python
import functools

import jax
import jax.numpy as jnp
from jax import lax
from jax.experimental import pallas as pl
from jax.experimental.pallas import tpu as pltpu
from jax.sharding import Mesh
from jax.sharding import PartitionSpec as P

D = 4096
HEAD_DIM = 64
GRID_W = 64
TOK = 256
EXPERTS = 32
CAP = 24
SLOTS = EXPERTS * CAP
HALF = SLOTS // 2
PAIRS = HEAD_DIM // 4
EXTRA = 8
EP = ("z", "c")
TP = ("y", "x")
CX = ("c", "x")
CY = ("c", "y")
BF = jnp.bfloat16
F32 = jnp.float32


def iota(shape, dim):
    return lax.broadcasted_iota(jnp.int32, shape, dim)


def mm(a, b):
    return jnp.dot(a, b, preferred_element_type=F32)


def column(row):
    n = row.shape[1]
    eye = iota((n, n), 0) == iota((n, n), 1)
    return jnp.sum(jnp.where(eye, jnp.broadcast_to(row, (n, n)), 0.0), axis=1, keepdims=True)


def slots_of(ids):
    e = iota((EXPERTS, TOK), 0)
    hits = [e == ids[k : k + 1] for k in range(2)]
    member = jnp.where(hits[0] | hits[1], 1.0, 0.0).astype(BF)
    before = jnp.where(iota((TOK, TOK), 0) < iota((TOK, TOK), 1), 1.0, 0.0).astype(BF)
    rank = mm(member, before)
    return [
        ids[k : k + 1] * CAP
        + jnp.sum(jnp.where(hits[k], rank, 0.0), axis=0, keepdims=True).astype(jnp.int32)
        for k in range(2)
    ]


def route_fn(ids, rows):
    first, second = slots_of(ids)
    s = iota((SLOTS, TOK), 0)
    chosen = jnp.where((s == first) | (s == second), 1.0, 0.0).astype(BF)
    return mm(chosen, rows).astype(BF)


def combine_fn(ids, group_weight, expert_weight, results):
    total = expert_weight[0:1] + expert_weight[1:2]
    out = None
    for k, slot in enumerate(slots_of(ids)):
        mix = column(group_weight * expert_weight[k : k + 1] / total)
        at = column(slot.astype(F32)).astype(jnp.int32)
        chosen = jnp.where(iota((TOK, SLOTS), 1) == at, 1.0, 0.0).astype(BF)
        part = mix * mm(chosen, results)
        out = part if out is None else out + part
    return out.astype(BF)


def rotated(x, gain, table):
    mean = jnp.sum(x * x, axis=0, keepdims=True) * (1.0 / HEAD_DIM)
    scaled = x * lax.rsqrt(mean + 1e-06) * gain
    parts = []
    for axis in range(2):
        lo = 2 * PAIRS * axis
        x1, x2 = scaled[lo : lo + PAIRS], scaled[lo + PAIRS : lo + 2 * PAIRS]
        cosine = table[PAIRS * axis : PAIRS * (axis + 1)]
        sine = table[PAIRS * (axis + 2) : PAIRS * (axis + 3)]
        parts += [x1 * cosine - x2 * sine, x2 * cosine + x1 * sine]
    return jnp.concatenate(parts, axis=0)


def rope_fn(queries, keys_t, values_t, table):
    q_t = queries.astype(F32).T
    q_gain, k_gain = table[64:128], table[128:192]
    heads = []
    for h in range(4):
        turned = rotated(q_t[h * HEAD_DIM : (h + 1) * HEAD_DIM], q_gain, table) * 0.125
        heads.append(jnp.concatenate([turned, jnp.zeros_like(turned)], axis=0).T.astype(BF))
    k = rotated(keys_t.astype(F32), k_gain, table)
    kv = jnp.concatenate([k, values_t.astype(F32)], axis=0).T.astype(BF)
    return heads, kv


def gate_up_fn(get_tokens, get_weight, put):
    ones = jnp.ones((EXTRA, 256), BF)
    rows = []
    sums = []
    for c in range(2):
        blocks = [get_tokens(4 * c + x) for x in range(4)]
        square = None
        for b in blocks:
            w = b.astype(F32)
            square = w * w if square is None else square + w * w
        total = None
        for _ in range(3):
            piece = square.astype(BF)
            square = square - piece.astype(F32)
            part = lax.dot_general(ones, piece, (((1,), (1,)), ((), ())), preferred_element_type=F32)
            total = part if total is None else total + part
        sums.append(total[0:1])
        rows.append(jnp.concatenate(blocks, axis=1))
    sums = jnp.concatenate(sums, axis=1) * 0.125
    high = sums.astype(BF).astype(F32)
    low = (sums - high) * 256.0
    pieces = [v[:, 256 * i : 256 * (i + 1)] for v in (high, low) for i in range(3)]
    extra = jnp.concatenate(pieces + [jnp.zeros((2, 256), F32)], axis=0)
    for s in range(4):
        w = get_weight(s)
        for c in range(2):
            put(s, c * HALF, mm(rows[c], w) * 32.0)
        put(s, SLOTS, extra)


def hidden_fn(get, put):
    sums = get(SLOTS, EXTRA)
    for i in range(3):
        square = (sums[i : i + 1] + sums[i + 3 : i + 4] * (1.0 / 256)) * (8.0 / D)
        inv = lax.rsqrt(column(square) + 1e-06) * (1.0 / 32)
        both = get(256 * i, 256)
        gate, up = both[:, :128] * inv, both[:, 128:] * inv
        put(256 * i, (gate / (1.0 + jnp.exp(-gate)) * up).astype(BF))


def down_fn(get_hidden, get_weight, put):
    rows = [
        [jnp.concatenate([get_hidden(2 * j, c), get_hidden(2 * j + 1, c)], axis=1) for j in range(2)]
        for c in range(2)
    ]
    for s in range(4):
        w = get_weight(s)
        for c in range(2):
            put(c, s, (mm(rows[c][0], w[:256]) + mm(rows[c][1], w[256:])).astype(BF))


def reduce_fn(get):
    return [
        sum(get(4 * c + y).astype(F32) for y in range(4)).astype(BF).reshape(16, CAP, 256)
        for c in range(2)
    ]


def route_kernel(ids, rows, out):
    out[...] = route_fn(ids[...], rows[...])


def combine_kernel(ids, gw, ew, res, out):
    out[...] = combine_fn(ids[...], gw[...], ew[...], res[...])


def rope_kernel(q, k, v, table, q_first, q_second, kv_out):
    heads, kv = rope_fn(q[...], k[...], v[...], table[...])
    for h in range(2):
        q_first[h] = heads[h]
        q_second[h] = heads[2 + h]
    kv_out[...] = kv


def pack_kernel(at, gate, up, down, *outs):
    for s in range(4):
        y = lax.rem(at[0] + s, 4)
        rows = pl.ds(pl.multiple_of(y * 1024, 1024), 1024)
        outs[s][0:1024, 0:128] = gate[rows, :]
        outs[s][0:1024, 128:256] = up[rows, :]
        outs[s][1024:1536, :] = down[pl.ds(pl.multiple_of(y * 512, 512), 512), :]


def gate_up_kernel(at, tokens, w0, w1, w2, w3, out):
    weights = (w0, w1, w2, w3)

    def put(s, row, value):
        out[lax.rem(at[0] + 4 - s, 4), row : row + value.shape[0], :] = value

    gate_up_fn(lambda i: tokens[i], lambda s: weights[s][0:1024, :], put)


def hidden_kernel(parts, out):
    def put(at, value):
        for y in range(4):
            out[y, at : at + value.shape[0], :] = value

    hidden_fn(lambda at, n: parts[at : at + n, :], put)


def down_kernel(at, hidden, w0, w1, w2, w3, out):
    weights = (w0, w1, w2, w3)

    def put(c, s, value):
        out[c, lax.rem(at[0] + 4 - s, 4)] = value

    down_fn(
        lambda x, c: hidden[x, c * HALF : (c + 1) * HALF, :],
        lambda s: weights[s][1024:1536, :],
        put,
    )


def reduce_kernel(parts, out):
    for c, value in enumerate(reduce_fn(lambda i: parts[i])):
        out[:, c] = value


KEYS = 1024


def attend_kernel(q, kv, out, scores):
    blocks = [(kv, i) for i in range(kv.shape[0] // KEYS)]

    def lanes(v, op):
        parts = [v[:, 128 * i : 128 * (i + 1)] for i in range(v.shape[1] // 128)]
        return functools.reduce(op, parts)

    def score(h, j):
        ref, i = blocks[j]
        s = lax.dot_general(
            q[h], ref[i * KEYS : (i + 1) * KEYS, :], (((1,), (1,)), ((), ())), preferred_element_type=F32
        )
        scores[h, :, j * KEYS : (j + 1) * KEYS] = s
        return lanes(s, jnp.maximum)

    def weigh(h, j, top):
        ref, i = blocks[j]
        p = jnp.exp(scores[h, :, j * KEYS : (j + 1) * KEYS] - top)
        return lanes(p, jnp.add), mm(p.astype(BF), ref[i * KEYS : (i + 1) * KEYS, :])

    n = len(blocks)
    top = functools.reduce(jnp.maximum, [score(0, j) for j in range(n)])
    results = []
    for h in range(2):
        top = jnp.max(top, axis=1, keepdims=True)
        following = total = summed = None
        for j in range(n):
            if h == 0:
                m = score(1, j)
                following = m if following is None else jnp.maximum(following, m)
            t, o = weigh(h, j, top)
            total = t if total is None else total + t
            summed = o if summed is None else summed + o
        top = following
        results.append(summed / jnp.sum(total, axis=1, keepdims=True))
    first = pltpu.roll(results[0], HEAD_DIM, axis=1)
    out[...] = jnp.where(iota(first.shape, 1) < HEAD_DIM, first, results[1]).astype(BF)


def call(kernel, outs, *args, flops=0, scratch=(), vmem=20, space=pltpu.VMEM):
    def spec(a):
        return pl.BlockSpec(memory_space=pltpu.SMEM if a.dtype == jnp.int32 and a.size == 1 else space)

    return pl.pallas_call(
        kernel,
        out_shape=outs,
        in_specs=[spec(a) for a in args],
        out_specs=jax.tree.map(lambda _: pl.BlockSpec(memory_space=space), outs),
        scratch_shapes=scratch,
        cost_estimate=pl.CostEstimate(flops=flops, transcendentals=0, bytes_accessed=0),
        compiler_params=pltpu.CompilerParams(vmem_limit_bytes=vmem << 20),
    )(*args)


def array(*shape, dtype=BF):
    return jax.ShapeDtypeStruct(shape, dtype)


def shifted(blocks, axis):
    return [b if s == 0 else lax.ppermute(b, axis, [(i, (i + s) % 4) for i in range(4)]) for s, b in enumerate(blocks)]


def exchange(a, axes):
    return lax.all_to_all(a, axes, split_axis=0, concat_axis=0, tiled=True)


def rope_table(query_gain, key_gain):
    position = lax.axis_index(EP) * TOK + jnp.arange(TOK, dtype=jnp.int32)
    grid_pos = jnp.stack([position // GRID_W, position % GRID_W], axis=0).astype(F32)
    frequency = 10000.0 ** (-jnp.arange(PAIRS, dtype=F32) / PAIRS)
    angles = (grid_pos[:, None, :] * frequency[None, :, None]).reshape(2 * PAIRS, TOK)
    gains = jnp.concatenate([query_gain, key_gain])
    return jnp.concatenate(
        [jnp.cos(angles), jnp.sin(angles), jnp.broadcast_to(gains[:, None], (2 * HEAD_DIM, TOK))], axis=0
    )


def attend(q, kv):
    scratch = [pltpu.VMEM((2, TOK, kv.shape[0]), F32)]
    return call(attend_kernel, array(TOK, 128), q, kv, flops=2200 << 20, scratch=scratch, vmem=36)


def on_device(
    queries,
    keys,
    values,
    query_gain,
    key_gain,
    moe_rows,
    route_ids,
    group_weight,
    expert_weight,
    expert_gate,
    expert_up,
    expert_down,
):
    tie = lax.optimization_barrier
    ids = route_ids.T
    routed = call(route_kernel, array(SLOTS, 256), ids, moe_rows, flops=4 << 20)
    arrived = exchange(routed.reshape(16, 2 * CAP, 256), "z")
    table = rope_table(query_gain, key_gain)
    *q_heads, kv = call(
        rope_kernel,
        (array(2, TOK, 128),) * 2 + (array(TOK, 128),),
        queries,
        keys.T,
        values.T,
        table,
        flops=4 << 20,
    )
    kv = lax.all_gather(kv, EP, axis=0, tiled=True)
    at = lax.axis_index("y").astype(jnp.int32).reshape(1)
    packed = call(pack_kernel, (array(1536, 256),) * 4, at, expert_gate[0], expert_up[0], expert_down[0])
    weights = shifted(packed, "y")
    arrived, q_heads = tie((arrived, q_heads))
    sent = arrived.reshape(16, 2, CAP, 256).transpose(1, 0, 2, 3).reshape(2, 1, HALF, 256)
    tokens = exchange(jnp.broadcast_to(sent, (2, 4, HALF, 256)).reshape(8, HALF, 256), CX)
    partial = call(
        gate_up_kernel, array(4, SLOTS + EXTRA, 256, dtype=F32), at, tokens, *weights, flops=1600 << 20
    ).astype(jnp.float16)
    products = exchange(partial, "y")
    hidden = call(
        hidden_kernel, array(4, SLOTS, 128), jnp.sum(products.astype(F32), axis=0), flops=8 << 20
    )
    hidden = exchange(hidden, "x")
    results = call(
        down_kernel, array(2, 4, HALF, 256), at, hidden, *weights, flops=800 << 20
    ).reshape(8, HALF, 256)
    results, q_heads = tie((results, q_heads))
    summands = exchange(results, CY)
    attended = jnp.concatenate([attend(q, kv) for q in q_heads], axis=1)
    summands, attended = tie((summands, attended))
    reduced = call(reduce_kernel, array(16, 2, CAP, 256), summands, flops=4 << 20)
    returned = exchange(reduced.reshape(16, 2 * CAP, 256), "z")
    moe_out = call(
        combine_kernel,
        array(TOK, 256),
        ids,
        group_weight.reshape(1, TOK),
        expert_weight.T,
        returned.reshape(SLOTS, 256),
        flops=8 << 20,
    )
    return (attended, moe_out)


def solution(mesh):
    torus = Mesh(mesh.devices.reshape(16, 2, 4, 4), ("z", "c", "y", "x"))

    return jax.shard_map(
        on_device,
        mesh=torus,
        in_specs=(
            P(EP, TP),
            P(EP, TP),
            P(EP, TP),
            P(),
            P(),
            P(EP, TP),
            P(EP, None),
            P(EP),
            P(EP, None),
            P(EP, None, TP),
            P(EP, None, TP),
            P(EP, None, TP),
        ),
        out_specs=(P(EP, TP), P(EP, TP)),
        check_vma=False,
    )
```

```python
import functools

import jax
import jax.numpy as jnp
from jax import lax
from jax.experimental import pallas as pl
from jax.experimental.pallas import tpu as pltpu
from jax.sharding import Mesh
from jax.sharding import PartitionSpec as P

D = 4096
HEAD_DIM = 64
GRID_W = 64
TOK = 256
EXPERTS = 32
CAP = 24
SLOTS = EXPERTS * CAP
HALF = SLOTS // 2
PAIRS = HEAD_DIM // 4
EXTRA = 8
EP = ("z", "c")
TP = ("y", "x")
CX = ("c", "x")
CY = ("c", "y")
BF = jnp.bfloat16
F32 = jnp.float32


def iota(shape, dim):
    return lax.broadcasted_iota(jnp.int32, shape, dim)


def mm(a, b):
    return jnp.dot(a, b, preferred_element_type=F32)


def column(row):
    n = row.shape[1]
    eye = iota((n, n), 0) == iota((n, n), 1)
    return jnp.sum(jnp.where(eye, jnp.broadcast_to(row, (n, n)), 0.0), axis=1, keepdims=True)


def slots_of(ids):
    e = iota((EXPERTS, TOK), 0)
    hits = [e == ids[k : k + 1] for k in range(2)]
    member = jnp.where(hits[0] | hits[1], 1.0, 0.0).astype(BF)
    before = jnp.where(iota((TOK, TOK), 0) < iota((TOK, TOK), 1), 1.0, 0.0).astype(BF)
    rank = mm(member, before)
    return [
        ids[k : k + 1] * CAP
        + jnp.sum(jnp.where(hits[k], rank, 0.0), axis=0, keepdims=True).astype(jnp.int32)
        for k in range(2)
    ]


def route_fn(ids, rows):
    first, second = slots_of(ids)
    s = iota((SLOTS, TOK), 0)
    chosen = jnp.where((s == first) | (s == second), 1.0, 0.0).astype(BF)
    return mm(chosen, rows).astype(BF)


def combine_fn(ids, group_weight, expert_weight, results):
    total = expert_weight[0:1] + expert_weight[1:2]
    out = None
    for k, slot in enumerate(slots_of(ids)):
        mix = column(group_weight * expert_weight[k : k + 1] / total)
        at = column(slot.astype(F32)).astype(jnp.int32)
        chosen = jnp.where(iota((TOK, SLOTS), 1) == at, 1.0, 0.0).astype(BF)
        part = mix * mm(chosen, results)
        out = part if out is None else out + part
    return out.astype(BF)


def rotated(x, gain, table):
    mean = jnp.sum(x * x, axis=0, keepdims=True) * (1.0 / HEAD_DIM)
    scaled = x * lax.rsqrt(mean + 1e-06) * gain
    parts = []
    for axis in range(2):
        lo = 2 * PAIRS * axis
        x1, x2 = scaled[lo : lo + PAIRS], scaled[lo + PAIRS : lo + 2 * PAIRS]
        cosine = table[PAIRS * axis : PAIRS * (axis + 1)]
        sine = table[PAIRS * (axis + 2) : PAIRS * (axis + 3)]
        parts += [x1 * cosine - x2 * sine, x2 * cosine + x1 * sine]
    return jnp.concatenate(parts, axis=0)


def query_fn(queries, table):
    q_t = queries.astype(F32).T
    heads = []
    for h in range(2):
        turned = rotated(q_t[h * HEAD_DIM : (h + 1) * HEAD_DIM], table[64:128], table) * 0.125
        heads.append(jnp.concatenate([turned, jnp.zeros_like(turned)], axis=0).T.astype(BF))
    return heads


def key_fn(keys_t, values_t, table):
    k = rotated(keys_t.astype(F32), table[128:192], table)
    return jnp.concatenate([k, values_t.astype(F32)], axis=0).T.astype(BF)


def gate_up_fn(get_tokens, get_weight, put):
    ones = jnp.ones((EXTRA, 256), BF)
    rows = []
    sums = []
    for c in range(2):
        blocks = [get_tokens(4 * c + x) for x in range(4)]
        square = None
        for b in blocks:
            w = b.astype(F32)
            square = w * w if square is None else square + w * w
        total = None
        for _ in range(3):
            piece = square.astype(BF)
            square = square - piece.astype(F32)
            part = lax.dot_general(ones, piece, (((1,), (1,)), ((), ())), preferred_element_type=F32)
            total = part if total is None else total + part
        sums.append(total[0:1])
        rows.append(jnp.concatenate(blocks, axis=1))
    sums = jnp.concatenate(sums, axis=1) * 0.125
    high = sums.astype(BF).astype(F32)
    low = (sums - high) * 256.0
    pieces = [v[:, 256 * i : 256 * (i + 1)] for v in (high, low) for i in range(3)]
    extra = jnp.concatenate(pieces + [jnp.zeros((2, 256), F32)], axis=0)
    for s in range(4):
        w = get_weight(s)
        for c in range(2):
            put(s, c * HALF, mm(rows[c], w) * 32.0)
        put(s, SLOTS, extra)


def hidden_fn(get, put):
    sums = get(SLOTS, EXTRA)
    for i in range(3):
        square = (sums[i : i + 1] + sums[i + 3 : i + 4] * (1.0 / 256)) * (8.0 / D)
        inv = lax.rsqrt(column(square) + 1e-06) * (1.0 / 32)
        both = get(256 * i, 256)
        gate, up = both[:, :128] * inv, both[:, 128:] * inv
        put(256 * i, (gate / (1.0 + jnp.exp(-gate)) * up).astype(BF))


def down_fn(get_hidden, get_weight, put):
    rows = [
        [jnp.concatenate([get_hidden(2 * j, c), get_hidden(2 * j + 1, c)], axis=1) for j in range(2)]
        for c in range(2)
    ]
    for s in range(4):
        w = get_weight(s)
        for c in range(2):
            put(c, s, (mm(rows[c][0], w[:256]) + mm(rows[c][1], w[256:])).astype(BF))


def reduce_fn(get):
    return [
        sum(get(4 * c + y).astype(F32) for y in range(4)).astype(BF).reshape(16, CAP, 256)
        for c in range(2)
    ]


def route_kernel(ids, rows, out):
    out[...] = route_fn(ids[...], rows[...])


def combine_kernel(ids, gw, ew, res, out):
    out[...] = combine_fn(ids[...], gw[...], ew[...], res[...])


def query_kernel(q, table, out):
    for h, head in enumerate(query_fn(q[...], table[...])):
        out[h] = head


def key_kernel(k, v, table, out):
    out[...] = key_fn(k[...], v[...], table[...])


def pack_kernel(at, gate, up, down, *outs):
    for s in range(4):
        y = lax.rem(at[0] + s, 4)
        rows = pl.ds(pl.multiple_of(y * 1024, 1024), 1024)
        outs[s][0:1024, 0:128] = gate[rows, :]
        outs[s][0:1024, 128:256] = up[rows, :]
        outs[s][1024:1536, :] = down[pl.ds(pl.multiple_of(y * 512, 512), 512), :]


def gate_up_kernel(at, tokens, w0, w1, w2, w3, out):
    weights = (w0, w1, w2, w3)

    def put(s, row, value):
        out[lax.rem(at[0] + 4 - s, 4), row : row + value.shape[0], :] = value

    gate_up_fn(lambda i: tokens[i], lambda s: weights[s][0:1024, :], put)


def hidden_kernel(parts, out):
    def put(at, value):
        for y in range(4):
            out[y, at : at + value.shape[0], :] = value

    hidden_fn(lambda at, n: parts[at : at + n, :], put)


def down_kernel(at, hidden, w0, w1, w2, w3, out):
    weights = (w0, w1, w2, w3)

    def put(c, s, value):
        out[c, lax.rem(at[0] + 4 - s, 4)] = value

    down_fn(
        lambda x, c: hidden[x, c * HALF : (c + 1) * HALF, :],
        lambda s: weights[s][1024:1536, :],
        put,
    )


def reduce_kernel(parts, out):
    for c, value in enumerate(reduce_fn(lambda i: parts[i])):
        out[:, c] = value


KEYS = 1024


def attend_kernel(q, own, other, out, scores):
    blocks = [(ref, i) for ref in (own, other) for i in range(ref.shape[0] // KEYS)]

    def lanes(v, op):
        parts = [v[:, 128 * i : 128 * (i + 1)] for i in range(v.shape[1] // 128)]
        return functools.reduce(op, parts)

    def score(h, j):
        ref, i = blocks[j]
        s = lax.dot_general(
            q[h], ref[i * KEYS : (i + 1) * KEYS, :], (((1,), (1,)), ((), ())), preferred_element_type=F32
        )
        scores[h, :, j * KEYS : (j + 1) * KEYS] = s
        return lanes(s, jnp.maximum)

    def weigh(h, j, top):
        ref, i = blocks[j]
        p = jnp.exp(scores[h, :, j * KEYS : (j + 1) * KEYS] - top)
        return lanes(p, jnp.add), mm(p.astype(BF), ref[i * KEYS : (i + 1) * KEYS, :])

    n = len(blocks)
    top = functools.reduce(jnp.maximum, [score(0, j) for j in range(n)])
    results = []
    for h in range(2):
        top = jnp.max(top, axis=1, keepdims=True)
        following = total = summed = None
        for j in range(n):
            if h == 0:
                m = score(1, j)
                following = m if following is None else jnp.maximum(following, m)
            t, o = weigh(h, j, top)
            total = t if total is None else total + t
            summed = o if summed is None else summed + o
        top = following
        results.append(summed / jnp.sum(total, axis=1, keepdims=True))
    first = pltpu.roll(results[0], HEAD_DIM, axis=1)
    out[...] = jnp.where(iota(first.shape, 1) < HEAD_DIM, first, results[1]).astype(BF)


def call(kernel, outs, *args, flops=0, scratch=(), vmem=20, space=pltpu.VMEM):
    def spec(a):
        return pl.BlockSpec(memory_space=pltpu.SMEM if a.dtype == jnp.int32 and a.size == 1 else space)

    return pl.pallas_call(
        kernel,
        out_shape=outs,
        in_specs=[spec(a) for a in args],
        out_specs=jax.tree.map(lambda _: pl.BlockSpec(memory_space=space), outs),
        scratch_shapes=scratch,
        cost_estimate=pl.CostEstimate(flops=flops, transcendentals=0, bytes_accessed=0),
        compiler_params=pltpu.CompilerParams(vmem_limit_bytes=vmem << 20),
    )(*args)


def array(*shape, dtype=BF):
    return jax.ShapeDtypeStruct(shape, dtype)


def shifted(blocks, axis):
    return [b if s == 0 else lax.ppermute(b, axis, [(i, (i + s) % 4) for i in range(4)]) for s, b in enumerate(blocks)]


def exchange(a, axes):
    return lax.all_to_all(a, axes, split_axis=0, concat_axis=0, tiled=True)


def rope_table(query_gain, key_gain):
    position = lax.axis_index(EP) * TOK + jnp.arange(TOK, dtype=jnp.int32)
    grid_pos = jnp.stack([position // GRID_W, position % GRID_W], axis=0).astype(F32)
    frequency = 10000.0 ** (-jnp.arange(PAIRS, dtype=F32) / PAIRS)
    angles = (grid_pos[:, None, :] * frequency[None, :, None]).reshape(2 * PAIRS, TOK)
    gains = jnp.concatenate([query_gain, key_gain])
    return jnp.concatenate(
        [jnp.cos(angles), jnp.sin(angles), jnp.broadcast_to(gains[:, None], (2 * HEAD_DIM, TOK))], axis=0
    )


def attend(q, own, other):
    scratch = [pltpu.VMEM((2, TOK, 2 * own.shape[0]), F32)]
    return call(attend_kernel, array(TOK, 128), q, own, other, flops=2200 << 20, scratch=scratch, vmem=36)


def spread(kv, shifts):
    moved = [lax.ppermute(kv, "z", [(i, (i + n) % 16) for i in range(16)]) for n in shifts]
    return jnp.concatenate([kv, *moved], axis=0)


def rotate_queries(q, table):
    return call(query_kernel, array(2, TOK, 128), q, table, flops=2 << 20)


def on_device(
    queries,
    keys,
    values,
    query_gain,
    key_gain,
    moe_rows,
    route_ids,
    group_weight,
    expert_weight,
    expert_gate,
    expert_up,
    expert_down,
):
    tie = lax.optimization_barrier
    ids = route_ids.T
    routed = call(route_kernel, array(SLOTS, 256), ids, moe_rows, flops=4 << 20)
    arrived = exchange(routed.reshape(16, 2 * CAP, 256), "z")
    table = rope_table(query_gain, key_gain)
    kv = call(key_kernel, array(TOK, 128), keys.T, values.T, table, flops=2 << 20)
    at = lax.axis_index("y").astype(jnp.int32).reshape(1)
    packed = call(pack_kernel, (array(1536, 256),) * 4, at, expert_gate[0], expert_up[0], expert_down[0])
    weights = shifted(packed, "y")
    arrived, kv, table = tie((arrived, kv, table))
    kv = spread(spread(kv, (4, 8, -4)), (1, 2, -1))
    q_heads = [rotate_queries(queries[:, :128], table), rotate_queries(queries[:, 128:], table)]
    sent = arrived.reshape(16, 2, CAP, 256).transpose(1, 0, 2, 3).reshape(2, 1, HALF, 256)
    tokens = exchange(jnp.broadcast_to(sent, (2, 4, HALF, 256)).reshape(8, HALF, 256), CX)
    partial = call(
        gate_up_kernel, array(4, SLOTS + EXTRA, 256, dtype=F32), at, tokens, *weights, flops=1600 << 20
    ).astype(jnp.float16)
    products = exchange(partial, "y")
    hidden = call(
        hidden_kernel, array(4, SLOTS, 128), jnp.sum(products.astype(F32), axis=0), flops=8 << 20
    )
    hidden = exchange(hidden, "x")
    results = call(
        down_kernel, array(2, 4, HALF, 256), at, hidden, *weights, flops=800 << 20
    ).reshape(8, HALF, 256)
    results, q_heads = tie((results, q_heads))
    summands = exchange(results, CY)
    other = lax.ppermute(kv, "c", [(0, 1), (1, 0)])
    attended = jnp.concatenate([attend(q, kv, other) for q in q_heads], axis=1)
    summands, attended = tie((summands, attended))
    reduced = call(reduce_kernel, array(16, 2, CAP, 256), summands, flops=4 << 20)
    returned = exchange(reduced.reshape(16, 2 * CAP, 256), "z")
    moe_out = call(
        combine_kernel,
        array(TOK, 256),
        ids,
        group_weight.reshape(1, TOK),
        expert_weight.T,
        returned.reshape(SLOTS, 256),
        flops=8 << 20,
    )
    return (attended, moe_out)


def solution(mesh):
    torus = Mesh(mesh.devices.reshape(16, 2, 4, 4), ("z", "c", "y", "x"))

    return jax.shard_map(
        on_device,
        mesh=torus,
        in_specs=(
            P(EP, TP),
            P(EP, TP),
            P(EP, TP),
            P(),
            P(),
            P(EP, TP),
            P(EP, None),
            P(EP),
            P(EP, None),
            P(EP, None, TP),
            P(EP, None, TP),
            P(EP, None, TP),
        ),
        out_specs=(P(EP, TP), P(EP, TP)),
        check_vma=False,
    )
```

```python
import functools

import jax
import jax.numpy as jnp
from jax import lax
from jax.experimental import pallas as pl
from jax.experimental.pallas import tpu as pltpu
from jax.sharding import Mesh
from jax.sharding import PartitionSpec as P

D = 4096
HEAD_DIM = 64
GRID_W = 64
TOK = 256
EXPERTS = 32
CAP = 24
SLOTS = EXPERTS * CAP
HALF = SLOTS // 2
PAIRS = HEAD_DIM // 4
EXTRA = 8
EP = ("z", "c")
TP = ("y", "x")
ACROSS = ("c", "y", "x")


def member(c, r, g):
    y, x = (r, g) if c == 0 else (g, r)
    return c * 16 + y * 4 + x


GATHER = [[member(c, r, g) for g in range(4)] for c in range(2) for r in range(4)]
REDUCE = [[member(c, r, g) for r in range(4)] for c in range(2) for g in range(4)]
BF = jnp.bfloat16
F32 = jnp.float32


def iota(shape, dim):
    return lax.broadcasted_iota(jnp.int32, shape, dim)


def mm(a, b):
    return jnp.dot(a, b, preferred_element_type=F32)


def column(row):
    n = row.shape[1]
    eye = iota((n, n), 0) == iota((n, n), 1)
    return jnp.sum(jnp.where(eye, jnp.broadcast_to(row, (n, n)), 0.0), axis=1, keepdims=True)


def slots_of(ids):
    e = iota((EXPERTS, TOK), 0)
    hits = [e == ids[k : k + 1] for k in range(2)]
    member = jnp.where(hits[0] | hits[1], 1.0, 0.0).astype(BF)
    before = jnp.where(iota((TOK, TOK), 0) < iota((TOK, TOK), 1), 1.0, 0.0).astype(BF)
    rank = mm(member, before)
    return [
        ids[k : k + 1] * CAP
        + jnp.sum(jnp.where(hits[k], rank, 0.0), axis=0, keepdims=True).astype(jnp.int32)
        for k in range(2)
    ]


def route_fn(ids, rows):
    first, second = slots_of(ids)
    s = iota((SLOTS, TOK), 0)
    chosen = jnp.where((s == first) | (s == second), 1.0, 0.0).astype(BF)
    return mm(chosen, rows).astype(BF)


def combine_fn(ids, group_weight, expert_weight, results):
    total = expert_weight[0:1] + expert_weight[1:2]
    out = None
    for k, slot in enumerate(slots_of(ids)):
        mix = column(group_weight * expert_weight[k : k + 1] / total)
        at = column(slot.astype(F32)).astype(jnp.int32)
        chosen = jnp.where(iota((TOK, SLOTS), 1) == at, 1.0, 0.0).astype(BF)
        part = mix * mm(chosen, results)
        out = part if out is None else out + part
    return out.astype(BF)


def rotated(x, gain, table):
    mean = jnp.sum(x * x, axis=0, keepdims=True) * (1.0 / HEAD_DIM)
    scaled = x * lax.rsqrt(mean + 1e-06) * gain
    parts = []
    for axis in range(2):
        lo = 2 * PAIRS * axis
        x1, x2 = scaled[lo : lo + PAIRS], scaled[lo + PAIRS : lo + 2 * PAIRS]
        cosine = table[PAIRS * axis : PAIRS * (axis + 1)]
        sine = table[PAIRS * (axis + 2) : PAIRS * (axis + 3)]
        parts += [x1 * cosine - x2 * sine, x2 * cosine + x1 * sine]
    return jnp.concatenate(parts, axis=0)


def rope_fn(queries, keys_t, values_t, table):
    q_t = queries.astype(F32).T
    q_gain, k_gain = table[64:128], table[128:192]
    heads = []
    for h in range(4):
        turned = rotated(q_t[h * HEAD_DIM : (h + 1) * HEAD_DIM], q_gain, table) * 0.125
        heads.append(jnp.concatenate([turned, jnp.zeros_like(turned)], axis=0).T.astype(BF))
    k = rotated(keys_t.astype(F32), k_gain, table)
    kv = jnp.concatenate([k, values_t.astype(F32)], axis=0).T.astype(BF)
    return heads, kv


def gate_up_fn(get_tokens, get_weight, put):
    ones = jnp.ones((EXTRA, 256), BF)
    rows = []
    sums = []
    for c in range(2):
        blocks = [get_tokens(4 * c + x) for x in range(4)]
        square = None
        for b in blocks:
            w = b.astype(F32)
            square = w * w if square is None else square + w * w
        total = None
        for _ in range(3):
            piece = square.astype(BF)
            square = square - piece.astype(F32)
            part = lax.dot_general(ones, piece, (((1,), (1,)), ((), ())), preferred_element_type=F32)
            total = part if total is None else total + part
        sums.append(total[0:1])
        rows.append(jnp.concatenate(blocks, axis=1))
    sums = jnp.concatenate(sums, axis=1) * 0.125
    high = sums.astype(BF).astype(F32)
    low = (sums - high) * 256.0
    pieces = [v[:, 256 * i : 256 * (i + 1)] for v in (high, low) for i in range(3)]
    extra = jnp.concatenate(pieces + [jnp.zeros((2, 256), F32)], axis=0)
    for s in range(4):
        w = get_weight(s)
        for c in range(2):
            put(s, c * HALF, mm(rows[c], w) * 32.0)
        put(s, SLOTS, extra)


def hidden_fn(get, put):
    sums = get(SLOTS, EXTRA)
    for i in range(3):
        square = (sums[i : i + 1] + sums[i + 3 : i + 4] * (1.0 / 256)) * (8.0 / D)
        inv = lax.rsqrt(column(square) + 1e-06) * (1.0 / 32)
        both = get(256 * i, 256)
        gate, up = both[:, :128] * inv, both[:, 128:] * inv
        put(256 * i, (gate / (1.0 + jnp.exp(-gate)) * up).astype(BF))


def down_fn(get_hidden, get_weight, put):
    rows = [
        [jnp.concatenate([get_hidden(2 * j, c), get_hidden(2 * j + 1, c)], axis=1) for j in range(2)]
        for c in range(2)
    ]
    for s in range(4):
        w = get_weight(s)
        for c in range(2):
            put(c, s, (mm(rows[c][0], w[:256]) + mm(rows[c][1], w[256:])).astype(BF))


def reduce_fn(get):
    return sum(get(r).astype(F32) for r in range(4)).astype(BF)


def route_kernel(ids, rows, out):
    out[...] = route_fn(ids[...], rows[...])


def combine_kernel(ids, gw, ew, res, out):
    out[...] = combine_fn(ids[...], gw[...], ew[...], res[...])


def rope_kernel(q, k, v, table, q_first, q_second, kv_out):
    heads, kv = rope_fn(q[...], k[...], v[...], table[...])
    for h in range(2):
        q_first[h] = heads[h]
        q_second[h] = heads[2 + h]
    kv_out[...] = kv


def pack_kernel(at, gate, up, down, *outs):
    for s in range(4):
        r = lax.rem(at[0] + s, 4)
        for j in range(4):
            part = r * at[1] + j * at[2]
            rows = pl.ds(pl.multiple_of(part * 256, 256), 256)
            outs[s][256 * j : 256 * (j + 1), 0:128] = gate[rows, :]
            outs[s][256 * j : 256 * (j + 1), 128:256] = up[rows, :]
            rows = pl.ds(pl.multiple_of(part * 128, 128), 128)
            outs[s][1024 + 128 * j : 1024 + 128 * (j + 1), :] = down[rows, :]


def gate_up_kernel(at, tokens, w0, w1, w2, w3, out):
    weights = (w0, w1, w2, w3)

    def put(s, row, value):
        out[lax.rem(at[0] + 4 - s, 4), row : row + value.shape[0], :] = value

    gate_up_fn(lambda i: tokens[i % 4, i // 4 * HALF : (i // 4 + 1) * HALF, :], lambda s: weights[s][0:1024, :], put)


def hidden_kernel(parts, out):
    def put(at, value):
        for y in range(4):
            out[y, at : at + value.shape[0], :] = value

    hidden_fn(lambda at, n: parts[at : at + n, :], put)


def down_kernel(at, hidden, w0, w1, w2, w3, out):
    weights = (w0, w1, w2, w3)

    def put(c, s, value):
        out[lax.rem(at[0] + 4 - s, 4), c * HALF : (c + 1) * HALF, :] = value

    down_fn(
        lambda x, c: hidden[x, c * HALF : (c + 1) * HALF, :],
        lambda s: weights[s][1024:1536, :],
        put,
    )


def reduce_kernel(parts, out):
    for c in range(2):
        out[c] = reduce_fn(lambda r: parts[r, c * HALF : (c + 1) * HALF, :])


KEYS = 1024


def attend_kernel(q, kv, out, scores):
    blocks = [(kv, i) for i in range(kv.shape[0] // KEYS)]

    def lanes(v, op):
        parts = [v[:, 128 * i : 128 * (i + 1)] for i in range(v.shape[1] // 128)]
        return functools.reduce(op, parts)

    def score(h, j):
        ref, i = blocks[j]
        s = lax.dot_general(
            q[h], ref[i * KEYS : (i + 1) * KEYS, :], (((1,), (1,)), ((), ())), preferred_element_type=F32
        )
        scores[h, :, j * KEYS : (j + 1) * KEYS] = s
        return lanes(s, jnp.maximum)

    def weigh(h, j, top):
        ref, i = blocks[j]
        p = jnp.exp(scores[h, :, j * KEYS : (j + 1) * KEYS] - top)
        return lanes(p, jnp.add), mm(p.astype(BF), ref[i * KEYS : (i + 1) * KEYS, :])

    n = len(blocks)
    top = functools.reduce(jnp.maximum, [score(0, j) for j in range(n)])
    results = []
    for h in range(2):
        top = jnp.max(top, axis=1, keepdims=True)
        following = total = summed = None
        for j in range(n):
            if h == 0:
                m = score(1, j)
                following = m if following is None else jnp.maximum(following, m)
            t, o = weigh(h, j, top)
            total = t if total is None else total + t
            summed = o if summed is None else summed + o
        top = following
        results.append(summed / jnp.sum(total, axis=1, keepdims=True))
    first = pltpu.roll(results[0], HEAD_DIM, axis=1)
    out[...] = jnp.where(iota(first.shape, 1) < HEAD_DIM, first, results[1]).astype(BF)


def call(kernel, outs, *args, flops=0, scratch=(), vmem=20, space=pltpu.VMEM):
    def spec(a):
        return pl.BlockSpec(memory_space=pltpu.SMEM if a.dtype == jnp.int32 and a.size == 3 else space)

    return pl.pallas_call(
        kernel,
        out_shape=outs,
        in_specs=[spec(a) for a in args],
        out_specs=jax.tree.map(lambda _: pl.BlockSpec(memory_space=space), outs),
        scratch_shapes=scratch,
        cost_estimate=pl.CostEstimate(flops=flops, transcendentals=0, bytes_accessed=0),
        compiler_params=pltpu.CompilerParams(vmem_limit_bytes=vmem << 20),
    )(*args)


def array(*shape, dtype=BF):
    return jax.ShapeDtypeStruct(shape, dtype)


def shifted(blocks):
    out = [blocks[0]]
    for s in range(1, 4):
        pairs = [(group[r], group[(r + s) % 4]) for group in REDUCE for r in range(4)]
        out.append(lax.ppermute(blocks[s], ACROSS, pairs))
    return out


def exchange(a, axes, groups=None):
    return lax.all_to_all(a, axes, split_axis=0, concat_axis=0, axis_index_groups=groups, tiled=True)


def rope_table(query_gain, key_gain):
    position = lax.axis_index(EP) * TOK + jnp.arange(TOK, dtype=jnp.int32)
    grid_pos = jnp.stack([position // GRID_W, position % GRID_W], axis=0).astype(F32)
    frequency = 10000.0 ** (-jnp.arange(PAIRS, dtype=F32) / PAIRS)
    angles = (grid_pos[:, None, :] * frequency[None, :, None]).reshape(2 * PAIRS, TOK)
    gains = jnp.concatenate([query_gain, key_gain])
    return jnp.concatenate(
        [jnp.cos(angles), jnp.sin(angles), jnp.broadcast_to(gains[:, None], (2 * HEAD_DIM, TOK))], axis=0
    )


def attend(q, kv):
    scratch = [pltpu.VMEM((2, TOK, kv.shape[0]), F32)]
    return call(attend_kernel, array(TOK, 128), q, kv, flops=2200 << 20, scratch=scratch, vmem=36)


def on_device(
    queries,
    keys,
    values,
    query_gain,
    key_gain,
    moe_rows,
    route_ids,
    group_weight,
    expert_weight,
    expert_gate,
    expert_up,
    expert_down,
):
    tie = lax.optimization_barrier
    ids = route_ids.T
    routed = call(route_kernel, array(SLOTS, 256), ids, moe_rows, flops=4 << 20)
    arrived = exchange(routed.reshape(16, 2 * CAP, 256), "z")
    table = rope_table(query_gain, key_gain)
    *q_heads, kv = call(
        rope_kernel,
        (array(2, TOK, 128),) * 2 + (array(TOK, 128),),
        queries,
        keys.T,
        values.T,
        table,
        flops=4 << 20,
    )
    kv = lax.all_gather(kv, EP, axis=0, tiled=True)
    flip = lax.axis_index("c")
    y, x = lax.axis_index("y"), lax.axis_index("x")
    at = jnp.stack([y + flip * (x - y), 4 - 3 * flip, 1 + 3 * flip]).astype(jnp.int32)
    packed = call(pack_kernel, (array(1536, 256),) * 4, at, expert_gate[0], expert_up[0], expert_down[0])
    weights = shifted(packed)
    arrived, q_heads = tie((arrived, q_heads))
    rows = arrived.reshape(16, 2, CAP, 256).transpose(1, 0, 2, 3).reshape(2, HALF, 256)
    rows = exchange(rows, "c").reshape(1, SLOTS, 256)
    tokens = exchange(jnp.broadcast_to(rows, (4, SLOTS, 256)), ACROSS, GATHER)
    partial = call(
        gate_up_kernel, array(4, SLOTS + EXTRA, 256, dtype=F32), at, tokens, *weights, flops=1600 << 20
    ).astype(jnp.float16)
    products = exchange(partial, ACROSS, REDUCE)
    hidden = call(
        hidden_kernel, array(4, SLOTS, 128), jnp.sum(products.astype(F32), axis=0), flops=8 << 20
    )
    hidden = exchange(hidden, ACROSS, GATHER)
    results = call(down_kernel, array(4, SLOTS, 256), at, hidden, *weights, flops=800 << 20)
    summands = exchange(results, ACROSS, REDUCE)
    reduced = call(reduce_kernel, array(2, HALF, 256), summands, flops=4 << 20)
    reduced = exchange(reduced, "c")
    reduced = reduced.reshape(2, 16, CAP, 256).transpose(1, 0, 2, 3).reshape(16, 2 * CAP, 256)
    reduced, q_heads = tie((reduced, q_heads))
    returned = exchange(reduced, "z")
    attended = jnp.concatenate([attend(q, kv) for q in q_heads], axis=1)
    returned, attended = tie((returned, attended))
    moe_out = call(
        combine_kernel,
        array(TOK, 256),
        ids,
        group_weight.reshape(1, TOK),
        expert_weight.T,
        returned.reshape(SLOTS, 256),
        flops=8 << 20,
    )
    return (attended, moe_out)


def solution(mesh):
    torus = Mesh(mesh.devices.reshape(16, 2, 4, 4), ("z", "c", "y", "x"))

    return jax.shard_map(
        on_device,
        mesh=torus,
        in_specs=(
            P(EP, TP),
            P(EP, TP),
            P(EP, TP),
            P(),
            P(),
            P(EP, TP),
            P(EP, None),
            P(EP),
            P(EP, None),
            P(EP, None, TP),
            P(EP, None, TP),
            P(EP, None, TP),
        ),
        out_specs=(P(EP, TP), P(EP, TP)),
        check_vma=False,
    )
```

```python
import functools

import jax
import jax.numpy as jnp
from jax import lax
from jax.experimental import pallas as pl
from jax.experimental.pallas import tpu as pltpu
from jax.sharding import Mesh
from jax.sharding import PartitionSpec as P

D = 4096
HEAD_DIM = 64
GRID_W = 64
TOK = 256
EXPERTS = 32
CAP = 24
SLOTS = EXPERTS * CAP
HALF = SLOTS // 2
PAIRS = HEAD_DIM // 4
EXTRA = 8
EP = ("z", "c")
TP = ("y", "x")
ACROSS = ("c", "y", "x")


def member(c, r, g):
    y, x = (r, g) if c == 0 else (g, r)
    return c * 16 + y * 4 + x


GATHER = [[member(c, r, g) for g in range(4)] for c in range(2) for r in range(4)]
REDUCE = [[member(c, r, g) for r in range(4)] for c in range(2) for g in range(4)]
BF = jnp.bfloat16
F32 = jnp.float32


def iota(shape, dim):
    return lax.broadcasted_iota(jnp.int32, shape, dim)


def mm(a, b):
    return jnp.dot(a, b, preferred_element_type=F32)


def column(row):
    n = row.shape[1]
    eye = iota((n, n), 0) == iota((n, n), 1)
    return jnp.sum(jnp.where(eye, jnp.broadcast_to(row, (n, n)), 0.0), axis=1, keepdims=True)


def slots_of(ids):
    e = iota((EXPERTS, TOK), 0)
    hits = [e == ids[k : k + 1] for k in range(2)]
    member = jnp.where(hits[0] | hits[1], 1.0, 0.0).astype(BF)
    before = jnp.where(iota((TOK, TOK), 0) < iota((TOK, TOK), 1), 1.0, 0.0).astype(BF)
    rank = mm(member, before)
    return [
        ids[k : k + 1] * CAP
        + jnp.sum(jnp.where(hits[k], rank, 0.0), axis=0, keepdims=True).astype(jnp.int32)
        for k in range(2)
    ]


def route_fn(ids, rows):
    first, second = slots_of(ids)
    s = iota((SLOTS, TOK), 0)
    chosen = jnp.where((s == first) | (s == second), 1.0, 0.0).astype(BF)
    return mm(chosen, rows).astype(BF)


def combine_fn(ids, group_weight, expert_weight, results):
    total = expert_weight[0:1] + expert_weight[1:2]
    out = None
    for k, slot in enumerate(slots_of(ids)):
        mix = column(group_weight * expert_weight[k : k + 1] / total)
        at = column(slot.astype(F32)).astype(jnp.int32)
        chosen = jnp.where(iota((TOK, SLOTS), 1) == at, 1.0, 0.0).astype(BF)
        part = mix * mm(chosen, results)
        out = part if out is None else out + part
    return out.astype(BF)


def rotated(x, gain, table):
    mean = jnp.sum(x * x, axis=0, keepdims=True) * (1.0 / HEAD_DIM)
    scaled = x * lax.rsqrt(mean + 1e-06) * gain
    parts = []
    for axis in range(2):
        lo = 2 * PAIRS * axis
        x1, x2 = scaled[lo : lo + PAIRS], scaled[lo + PAIRS : lo + 2 * PAIRS]
        cosine = table[PAIRS * axis : PAIRS * (axis + 1)]
        sine = table[PAIRS * (axis + 2) : PAIRS * (axis + 3)]
        parts += [x1 * cosine - x2 * sine, x2 * cosine + x1 * sine]
    return jnp.concatenate(parts, axis=0)


def query_fn(queries, table):
    turned = rotated(queries.astype(F32).T, table[64:128], table) * 0.125
    return jnp.concatenate([turned, jnp.zeros_like(turned)], axis=0).T.astype(BF)


def key_fn(keys_t, values_t, table):
    k = rotated(keys_t.astype(F32), table[128:192], table)
    return jnp.concatenate([k, values_t.astype(F32)], axis=0).T.astype(BF)


def gate_up_fn(get_tokens, get_weight, put):
    ones = jnp.ones((EXTRA, 256), BF)
    rows = []
    sums = []
    for c in range(2):
        blocks = [get_tokens(4 * c + x) for x in range(4)]
        square = None
        for b in blocks:
            w = b.astype(F32)
            square = w * w if square is None else square + w * w
        total = None
        for _ in range(3):
            piece = square.astype(BF)
            square = square - piece.astype(F32)
            part = lax.dot_general(ones, piece, (((1,), (1,)), ((), ())), preferred_element_type=F32)
            total = part if total is None else total + part
        sums.append(total[0:1])
        rows.append(jnp.concatenate(blocks, axis=1))
    sums = jnp.concatenate(sums, axis=1) * 0.125
    high = sums.astype(BF).astype(F32)
    low = (sums - high) * 256.0
    pieces = [v[:, 256 * i : 256 * (i + 1)] for v in (high, low) for i in range(3)]
    extra = jnp.concatenate(pieces + [jnp.zeros((2, 256), F32)], axis=0)
    for s in range(4):
        w = get_weight(s)
        for c in range(2):
            put(s, c * HALF, mm(rows[c], w) * 32.0)
        put(s, SLOTS, extra)


def hidden_fn(get, put):
    sums = get(SLOTS, EXTRA)
    for i in range(3):
        square = (sums[i : i + 1] + sums[i + 3 : i + 4] * (1.0 / 256)) * (8.0 / D)
        inv = lax.rsqrt(column(square) + 1e-06) * (1.0 / 32)
        both = get(256 * i, 256)
        gate, up = both[:, :128] * inv, both[:, 128:] * inv
        put(256 * i, (gate / (1.0 + jnp.exp(-gate)) * up).astype(BF))


def down_fn(get_hidden, get_weight, put):
    rows = [
        [jnp.concatenate([get_hidden(2 * j, c), get_hidden(2 * j + 1, c)], axis=1) for j in range(2)]
        for c in range(2)
    ]
    for s in range(4):
        w = get_weight(s)
        for c in range(2):
            put(c, s, (mm(rows[c][0], w[:256]) + mm(rows[c][1], w[256:])).astype(BF))


def reduce_fn(get):
    return sum(get(r).astype(F32) for r in range(4)).astype(BF)


def route_kernel(ids, rows, out):
    out[...] = route_fn(ids[...], rows[...])


def combine_kernel(ids, gw, ew, res, out):
    out[...] = combine_fn(ids[...], gw[...], ew[...], res[...])


def query_kernel(q, table, out, *, head):
    out[...] = query_fn(q[:, head * HEAD_DIM : (head + 1) * HEAD_DIM], table[...])


def key_kernel(k, v, table, out):
    out[...] = key_fn(k[...], v[...], table[...])


def pack_kernel(at, gate, up, down, *outs):
    for s in range(4):
        r = lax.rem(at[0] + s, 4)
        for j in range(4):
            part = r * at[1] + j * at[2]
            rows = pl.ds(pl.multiple_of(part * 256, 256), 256)
            outs[s][256 * j : 256 * (j + 1), 0:128] = gate[rows, :]
            outs[s][256 * j : 256 * (j + 1), 128:256] = up[rows, :]
            rows = pl.ds(pl.multiple_of(part * 128, 128), 128)
            outs[s][1024 + 128 * j : 1024 + 128 * (j + 1), :] = down[rows, :]


def gate_up_kernel(at, tokens, w0, w1, w2, w3, out):
    weights = (w0, w1, w2, w3)

    def put(s, row, value):
        out[lax.rem(at[0] + 4 - s, 4), row : row + value.shape[0], :] = value

    gate_up_fn(lambda i: tokens[i % 4, i // 4 * HALF : (i // 4 + 1) * HALF, :], lambda s: weights[s][0:1024, :], put)


def hidden_kernel(parts, out):
    def put(at, value):
        for y in range(4):
            out[y, at : at + value.shape[0], :] = value

    hidden_fn(lambda at, n: parts[at : at + n, :], put)


def down_kernel(at, hidden, w0, w1, w2, w3, out):
    weights = (w0, w1, w2, w3)

    def put(c, s, value):
        out[lax.rem(at[0] + 4 - s, 4), c * HALF : (c + 1) * HALF, :] = value

    down_fn(
        lambda x, c: hidden[x, c * HALF : (c + 1) * HALF, :],
        lambda s: weights[s][1024:1536, :],
        put,
    )


def reduce_kernel(parts, out):
    for c in range(2):
        out[c] = reduce_fn(lambda r: parts[r, c * HALF : (c + 1) * HALF, :])


KEYS = 1024


def attend_kernel(q_first, q_second, own, other, out, scores):
    q = (q_first, q_second)
    blocks = [(ref, i) for ref in (own, other) for i in range(ref.shape[0] // KEYS)]

    def lanes(v, op):
        parts = [v[:, 128 * i : 128 * (i + 1)] for i in range(v.shape[1] // 128)]
        return functools.reduce(op, parts)

    def score(h, j):
        ref, i = blocks[j]
        s = lax.dot_general(
            q[h][...], ref[i * KEYS : (i + 1) * KEYS, :], (((1,), (1,)), ((), ())), preferred_element_type=F32
        )
        scores[h, :, j * KEYS : (j + 1) * KEYS] = s
        return lanes(s, jnp.maximum)

    def weigh(h, j, top):
        ref, i = blocks[j]
        p = jnp.exp(scores[h, :, j * KEYS : (j + 1) * KEYS] - top)
        return lanes(p, jnp.add), mm(p.astype(BF), ref[i * KEYS : (i + 1) * KEYS, :])

    n = len(blocks)
    top = functools.reduce(jnp.maximum, [score(0, j) for j in range(n)])
    results = []
    for h in range(2):
        top = jnp.max(top, axis=1, keepdims=True)
        following = total = summed = None
        for j in range(n):
            if h == 0:
                m = score(1, j)
                following = m if following is None else jnp.maximum(following, m)
            t, o = weigh(h, j, top)
            total = t if total is None else total + t
            summed = o if summed is None else summed + o
        top = following
        results.append(summed / jnp.sum(total, axis=1, keepdims=True))
    first = pltpu.roll(results[0], HEAD_DIM, axis=1)
    out[...] = jnp.where(iota(first.shape, 1) < HEAD_DIM, first, results[1]).astype(BF)


def call(kernel, outs, *args, flops=0, scratch=(), vmem=20, space=pltpu.VMEM):
    def spec(a):
        return pl.BlockSpec(memory_space=pltpu.SMEM if a.dtype == jnp.int32 and a.size == 3 else space)

    return pl.pallas_call(
        kernel,
        out_shape=outs,
        in_specs=[spec(a) for a in args],
        out_specs=jax.tree.map(lambda _: pl.BlockSpec(memory_space=space), outs),
        scratch_shapes=scratch,
        cost_estimate=pl.CostEstimate(flops=flops, transcendentals=0, bytes_accessed=0),
        compiler_params=pltpu.CompilerParams(vmem_limit_bytes=vmem << 20),
    )(*args)


def array(*shape, dtype=BF):
    return jax.ShapeDtypeStruct(shape, dtype)


def shifted(blocks):
    out = [blocks[0]]
    for s in range(1, 4):
        pairs = [(group[r], group[(r + s) % 4]) for group in REDUCE for r in range(4)]
        out.append(lax.ppermute(blocks[s], ACROSS, pairs))
    return out


def exchange(a, axes, groups=None):
    return lax.all_to_all(a, axes, split_axis=0, concat_axis=0, axis_index_groups=groups, tiled=True)


def rope_table(query_gain, key_gain):
    position = lax.axis_index(EP) * TOK + jnp.arange(TOK, dtype=jnp.int32)
    grid_pos = jnp.stack([position // GRID_W, position % GRID_W], axis=0).astype(F32)
    frequency = 10000.0 ** (-jnp.arange(PAIRS, dtype=F32) / PAIRS)
    angles = (grid_pos[:, None, :] * frequency[None, :, None]).reshape(2 * PAIRS, TOK)
    gains = jnp.concatenate([query_gain, key_gain])
    return jnp.concatenate(
        [jnp.cos(angles), jnp.sin(angles), jnp.broadcast_to(gains[:, None], (2 * HEAD_DIM, TOK))], axis=0
    )


def attend(q, own, other):
    scratch = [pltpu.VMEM((2, TOK, 2 * own.shape[0]), F32)]
    return call(attend_kernel, array(TOK, 128), *q, own, other, flops=2200 << 20, scratch=scratch, vmem=32)


def moved(kv, shift):
    return lax.ppermute(kv, "z", [(i, (i + shift) % 16) for i in range(16)])


def join_kernel(a, b, out):
    out[: a.shape[0]] = a[...]
    out[a.shape[0] :] = b[...]


def rotate_queries(q, table, head):
    kernel = functools.partial(query_kernel, head=head)
    return call(kernel, array(TOK, 128), q, table, flops=2 << 20)


def on_device(
    queries,
    keys,
    values,
    query_gain,
    key_gain,
    moe_rows,
    route_ids,
    group_weight,
    expert_weight,
    expert_gate,
    expert_up,
    expert_down,
):
    tie = lax.optimization_barrier
    ids = route_ids.T
    routed = call(route_kernel, array(SLOTS, 256), ids, moe_rows, flops=4 << 20)
    arrived = exchange(routed.reshape(16, 2 * CAP, 256), "z")
    table = rope_table(query_gain, key_gain)
    kv = call(key_kernel, array(TOK, 128), keys.T, values.T, table, flops=2 << 20)
    flip = lax.axis_index("c")
    y, x = lax.axis_index("y"), lax.axis_index("x")
    at = jnp.stack([y + flip * (x - y), 4 - 3 * flip, 1 + 3 * flip]).astype(jnp.int32)
    packed = call(pack_kernel, (array(1536, 256),) * 4, at, expert_gate[0], expert_up[0], expert_down[0])
    weights = shifted(packed)
    arrived, kv, table = tie((arrived, kv, table))
    for shift in (8, 4, -2):
        kv = jnp.concatenate([kv, moved(kv, shift)], axis=0)
    last = moved(kv, 1)
    q_heads = [rotate_queries(queries, table, head) for head in range(4)]
    rows = arrived.reshape(16, 2, CAP, 256).transpose(1, 0, 2, 3).reshape(2, HALF, 256)
    rows = exchange(rows, "c").reshape(1, SLOTS, 256)
    tokens = exchange(jnp.broadcast_to(rows, (4, SLOTS, 256)), ACROSS, GATHER)
    partial = call(
        gate_up_kernel, array(4, SLOTS + EXTRA, 256, dtype=F32), at, tokens, *weights, flops=1600 << 20
    ).astype(jnp.float16)
    products = exchange(partial, ACROSS, REDUCE)
    hidden = call(
        hidden_kernel, array(4, SLOTS, 128), jnp.sum(products.astype(F32), axis=0), flops=8 << 20
    )
    hidden = exchange(hidden, ACROSS, GATHER)
    results = call(down_kernel, array(4, SLOTS, 256), at, hidden, *weights, flops=800 << 20)
    summands = exchange(results, ACROSS, REDUCE)
    reduced = call(reduce_kernel, array(2, HALF, 256), summands, flops=4 << 20)
    reduced = exchange(reduced, "c")
    reduced = reduced.reshape(2, 16, CAP, 256).transpose(1, 0, 2, 3).reshape(16, 2 * CAP, 256)
    reduced, q_heads, kv = tie((reduced, q_heads, kv))
    returned = exchange(reduced, "z")
    kv = call(join_kernel, array(16 * TOK, 128), kv, last)
    other = lax.ppermute(kv, "c", [(0, 1), (1, 0)])
    attended = jnp.concatenate([attend(q_heads[i : i + 2], kv, other) for i in (0, 2)], axis=1)
    returned, attended = tie((returned, attended))
    moe_out = call(
        combine_kernel,
        array(TOK, 256),
        ids,
        group_weight.reshape(1, TOK),
        expert_weight.T,
        returned.reshape(SLOTS, 256),
        flops=8 << 20,
    )
    return (attended, moe_out)


def solution(mesh):
    torus = Mesh(mesh.devices.reshape(16, 2, 4, 4), ("z", "c", "y", "x"))

    return jax.shard_map(
        on_device,
        mesh=torus,
        in_specs=(
            P(EP, TP),
            P(EP, TP),
            P(EP, TP),
            P(),
            P(),
            P(EP, TP),
            P(EP, None),
            P(EP),
            P(EP, None),
            P(EP, None, TP),
            P(EP, None, TP),
            P(EP, None, TP),
        ),
        out_specs=(P(EP, TP), P(EP, TP)),
        check_vma=False,
    )
```

```python
import functools

import jax
import jax.numpy as jnp
from jax import lax
from jax.experimental import pallas as pl
from jax.experimental.pallas import tpu as pltpu
from jax.sharding import Mesh
from jax.sharding import PartitionSpec as P

D = 4096
HEAD_DIM = 64
GRID_W = 64
TOK = 256
EXPERTS = 32
CAP = 24
SLOTS = EXPERTS * CAP
HALF = SLOTS // 2
PAIRS = HEAD_DIM // 4
EXTRA = 8
EP = ("z", "c")
TP = ("y", "x")
ACROSS = ("c", "y", "x")


def member(c, r, g):
    y, x = (r, g) if c == 0 else (g, r)
    return c * 16 + y * 4 + x


GATHER = [[member(c, r, g) for g in range(4)] for c in range(2) for r in range(4)]
REDUCE = [[member(c, r, g) for r in range(4)] for c in range(2) for g in range(4)]
BF = jnp.bfloat16
F32 = jnp.float32


def iota(shape, dim):
    return lax.broadcasted_iota(jnp.int32, shape, dim)


def mm(a, b):
    return jnp.dot(a, b, preferred_element_type=F32)


def column(row):
    n = row.shape[1]
    eye = iota((n, n), 0) == iota((n, n), 1)
    return jnp.sum(jnp.where(eye, jnp.broadcast_to(row, (n, n)), 0.0), axis=1, keepdims=True)


def slots_of(ids):
    e = iota((EXPERTS, TOK), 0)
    hits = [e == ids[k : k + 1] for k in range(2)]
    member = jnp.where(hits[0] | hits[1], 1.0, 0.0).astype(BF)
    before = jnp.where(iota((TOK, TOK), 0) < iota((TOK, TOK), 1), 1.0, 0.0).astype(BF)
    rank = mm(member, before)
    return [
        ids[k : k + 1] * CAP
        + jnp.sum(jnp.where(hits[k], rank, 0.0), axis=0, keepdims=True).astype(jnp.int32)
        for k in range(2)
    ]


def route_fn(ids, rows):
    first, second = slots_of(ids)
    s = iota((SLOTS, TOK), 0)
    chosen = jnp.where((s == first) | (s == second), 1.0, 0.0).astype(BF)
    return mm(chosen, rows).astype(BF)


def combine_fn(ids, group_weight, expert_weight, results):
    total = expert_weight[0:1] + expert_weight[1:2]
    out = None
    for k, slot in enumerate(slots_of(ids)):
        mix = column(group_weight * expert_weight[k : k + 1] / total)
        at = column(slot.astype(F32)).astype(jnp.int32)
        chosen = jnp.where(iota((TOK, SLOTS), 1) == at, 1.0, 0.0).astype(BF)
        part = mix * mm(chosen, results)
        out = part if out is None else out + part
    return out.astype(BF)


def rotated(x, gain, table):
    mean = jnp.sum(x * x, axis=0, keepdims=True) * (1.0 / HEAD_DIM)
    scaled = x * lax.rsqrt(mean + 1e-06) * gain
    parts = []
    for axis in range(2):
        lo = 2 * PAIRS * axis
        x1, x2 = scaled[lo : lo + PAIRS], scaled[lo + PAIRS : lo + 2 * PAIRS]
        cosine = table[PAIRS * axis : PAIRS * (axis + 1)]
        sine = table[PAIRS * (axis + 2) : PAIRS * (axis + 3)]
        parts += [x1 * cosine - x2 * sine, x2 * cosine + x1 * sine]
    return jnp.concatenate(parts, axis=0)


def query_fn(queries, table):
    turned = rotated(queries.astype(F32).T, table[64:128], table) * 0.125
    return jnp.concatenate([turned, jnp.zeros_like(turned)], axis=0).T.astype(BF)


def key_fn(keys_t, values_t, table):
    k = rotated(keys_t.astype(F32), table[128:192], table)
    return jnp.concatenate([k, values_t.astype(F32)], axis=0).T.astype(BF)


def gate_up_fn(get_tokens, get_weight, put):
    ones = jnp.ones((EXTRA, 256), BF)
    rows = []
    sums = []
    for c in range(2):
        blocks = [get_tokens(4 * c + x) for x in range(4)]
        square = None
        for b in blocks:
            w = b.astype(F32)
            square = w * w if square is None else square + w * w
        total = None
        for _ in range(3):
            piece = square.astype(BF)
            square = square - piece.astype(F32)
            part = lax.dot_general(ones, piece, (((1,), (1,)), ((), ())), preferred_element_type=F32)
            total = part if total is None else total + part
        sums.append(total[0:1])
        rows.append(jnp.concatenate(blocks, axis=1))
    sums = jnp.concatenate(sums, axis=1) * 0.125
    high = sums.astype(BF).astype(F32)
    low = (sums - high) * 256.0
    pieces = [v[:, 256 * i : 256 * (i + 1)] for v in (high, low) for i in range(3)]
    extra = jnp.concatenate(pieces + [jnp.zeros((2, 256), F32)], axis=0)
    for s in range(4):
        w = get_weight(s)
        for c in range(2):
            put(s, c * HALF, mm(rows[c], w) * 32.0)
        put(s, SLOTS, extra)


def hidden_fn(get, put):
    sums = get(SLOTS, EXTRA)
    for i in range(3):
        square = (sums[i : i + 1] + sums[i + 3 : i + 4] * (1.0 / 256)) * (8.0 / D)
        inv = lax.rsqrt(column(square) + 1e-06) * (1.0 / 32)
        both = get(256 * i, 256)
        gate, up = both[:, :128] * inv, both[:, 128:] * inv
        put(256 * i, (gate / (1.0 + jnp.exp(-gate)) * up).astype(BF))


def down_fn(get_hidden, get_weight, put):
    rows = [
        [jnp.concatenate([get_hidden(2 * j, c), get_hidden(2 * j + 1, c)], axis=1) for j in range(2)]
        for c in range(2)
    ]
    for s in range(4):
        w = get_weight(s)
        for c in range(2):
            put(c, s, (mm(rows[c][0], w[:256]) + mm(rows[c][1], w[256:])).astype(BF))


def reduce_fn(get):
    return sum(get(r).astype(F32) for r in range(4)).astype(BF)


def route_kernel(ids, rows, out):
    out[...] = route_fn(ids[...], rows[...])


def combine_kernel(ids, gw, ew, res, out):
    out[...] = combine_fn(ids[...], gw[...], ew[...], res[...])


def query_kernel(q, table, out, *, head):
    out[...] = query_fn(q[:, head * HEAD_DIM : (head + 1) * HEAD_DIM], table[...])


def key_kernel(k, v, table, out):
    out[...] = key_fn(k[...], v[...], table[...])


def pack_kernel(at, gate, up, down, *outs):
    for s in range(4):
        r = lax.rem(at[0] + s, 4)
        for j in range(4):
            part = r * at[1] + j * at[2]
            rows = pl.ds(pl.multiple_of(part * 256, 256), 256)
            outs[s][256 * j : 256 * (j + 1), 0:128] = gate[rows, :]
            outs[s][256 * j : 256 * (j + 1), 128:256] = up[rows, :]
            rows = pl.ds(pl.multiple_of(part * 128, 128), 128)
            outs[s][1024 + 128 * j : 1024 + 128 * (j + 1), :] = down[rows, :]


def gate_up_kernel(at, tokens, w0, w1, w2, w3, out):
    weights = (w0, w1, w2, w3)

    def put(s, row, value):
        out[lax.rem(at[0] + 4 - s, 4), row : row + value.shape[0], :] = value

    gate_up_fn(lambda i: tokens[i % 4, i // 4 * HALF : (i // 4 + 1) * HALF, :], lambda s: weights[s][0:1024, :], put)


def hidden_kernel(parts, out):
    def put(at, value):
        for y in range(4):
            out[y, at : at + value.shape[0], :] = value

    hidden_fn(lambda at, n: parts[at : at + n, :], put)


def down_kernel(at, hidden, w0, w1, w2, w3, out):
    weights = (w0, w1, w2, w3)

    def put(c, s, value):
        out[lax.rem(at[0] + 4 - s, 4), c * HALF : (c + 1) * HALF, :] = value

    down_fn(
        lambda x, c: hidden[x, c * HALF : (c + 1) * HALF, :],
        lambda s: weights[s][1024:1536, :],
        put,
    )


def reduce_kernel(parts, out):
    for c in range(2):
        out[c] = reduce_fn(lambda r: parts[r, c * HALF : (c + 1) * HALF, :])


KEYS = 1024


def attend_kernel(q0, q1, q2, q3, own, other, out, scores):
    q = (q0, q1, q2, q3)
    blocks = [(ref, i) for ref in (own, other) for i in range(ref.shape[0] // KEYS)]

    def lanes(v, op):
        parts = [v[:, 128 * i : 128 * (i + 1)] for i in range(v.shape[1] // 128)]
        return functools.reduce(op, parts)

    def score(h, j):
        ref, i = blocks[j]
        s = lax.dot_general(
            q[h][...], ref[i * KEYS : (i + 1) * KEYS, :], (((1,), (1,)), ((), ())), preferred_element_type=F32
        )
        scores[h % 2, :, j * KEYS : (j + 1) * KEYS] = s
        return lanes(s, jnp.maximum)

    def weigh(h, j, top):
        ref, i = blocks[j]
        p = jnp.exp(scores[h % 2, :, j * KEYS : (j + 1) * KEYS] - top)
        return lanes(p, jnp.add), mm(p.astype(BF), ref[i * KEYS : (i + 1) * KEYS, :])

    n = len(blocks)
    top = functools.reduce(jnp.maximum, [score(0, j) for j in range(n)])
    even = None
    for h in range(len(q)):
        top = jnp.max(top, axis=1, keepdims=True)
        following = total = summed = None
        for j in range(n):
            if h + 1 < len(q):
                m = score(h + 1, j)
                following = m if following is None else jnp.maximum(following, m)
            t, o = weigh(h, j, top)
            total = t if total is None else total + t
            summed = o if summed is None else summed + o
        top = following
        result = summed / jnp.sum(total, axis=1, keepdims=True)
        if h % 2 == 0:
            even = pltpu.roll(result, HEAD_DIM, axis=1)
        else:
            pair = jnp.where(iota(result.shape, 1) < HEAD_DIM, even, result)
            out[:, HEAD_DIM * (h - 1) : HEAD_DIM * (h + 1)] = pair.astype(BF)


def call(kernel, outs, *args, flops=0, scratch=(), vmem=20, space=pltpu.VMEM):
    def spec(a):
        return pl.BlockSpec(memory_space=pltpu.SMEM if a.dtype == jnp.int32 and a.size == 3 else space)

    return pl.pallas_call(
        kernel,
        out_shape=outs,
        in_specs=[spec(a) for a in args],
        out_specs=jax.tree.map(lambda _: pl.BlockSpec(memory_space=space), outs),
        scratch_shapes=scratch,
        cost_estimate=pl.CostEstimate(flops=flops, transcendentals=0, bytes_accessed=0),
        compiler_params=pltpu.CompilerParams(vmem_limit_bytes=vmem << 20),
    )(*args)


def array(*shape, dtype=BF):
    return jax.ShapeDtypeStruct(shape, dtype)


def shifted(blocks):
    out = [blocks[0]]
    for s in range(1, 4):
        pairs = [(group[r], group[(r + s) % 4]) for group in REDUCE for r in range(4)]
        out.append(lax.ppermute(blocks[s], ACROSS, pairs))
    return out


def exchange(a, axes, groups=None):
    return lax.all_to_all(a, axes, split_axis=0, concat_axis=0, axis_index_groups=groups, tiled=True)


def rope_table(query_gain, key_gain):
    position = lax.axis_index(EP) * TOK + jnp.arange(TOK, dtype=jnp.int32)
    grid_pos = jnp.stack([position // GRID_W, position % GRID_W], axis=0).astype(F32)
    frequency = 10000.0 ** (-jnp.arange(PAIRS, dtype=F32) / PAIRS)
    angles = (grid_pos[:, None, :] * frequency[None, :, None]).reshape(2 * PAIRS, TOK)
    gains = jnp.concatenate([query_gain, key_gain])
    return jnp.concatenate(
        [jnp.cos(angles), jnp.sin(angles), jnp.broadcast_to(gains[:, None], (2 * HEAD_DIM, TOK))], axis=0
    )


def attend(q, own, other):
    scratch = [pltpu.VMEM((2, TOK, 2 * own.shape[0]), F32)]
    return call(attend_kernel, array(TOK, 256), *q, own, other, flops=4400 << 20, scratch=scratch, vmem=32)


def moved(kv, shift):
    return lax.ppermute(kv, "z", [(i, (i + shift) % 16) for i in range(16)])


def join_kernel(a, b, out):
    out[: a.shape[0]] = a[...]
    out[a.shape[0] :] = b[...]


def rotate_queries(q, table, head):
    kernel = functools.partial(query_kernel, head=head)
    return call(kernel, array(TOK, 128), q, table, flops=2 << 20)


def on_device(
    queries,
    keys,
    values,
    query_gain,
    key_gain,
    moe_rows,
    route_ids,
    group_weight,
    expert_weight,
    expert_gate,
    expert_up,
    expert_down,
):
    tie = lax.optimization_barrier
    ids = route_ids.T
    routed = call(route_kernel, array(SLOTS, 256), ids, moe_rows, flops=4 << 20)
    arrived = exchange(routed.reshape(16, 2 * CAP, 256), "z")
    table = rope_table(query_gain, key_gain)
    kv = call(key_kernel, array(TOK, 128), keys.T, values.T, table, flops=2 << 20)
    flip = lax.axis_index("c")
    y, x = lax.axis_index("y"), lax.axis_index("x")
    at = jnp.stack([y + flip * (x - y), 4 - 3 * flip, 1 + 3 * flip]).astype(jnp.int32)
    packed = call(pack_kernel, (array(1536, 256),) * 4, at, expert_gate[0], expert_up[0], expert_down[0])
    weights = shifted(packed)
    arrived, kv, table = tie((arrived, kv, table))
    for shift in (8, 4, -2):
        kv = jnp.concatenate([kv, moved(kv, shift)], axis=0)
    last = moved(kv, 1)
    q_heads = [rotate_queries(queries, table, head) for head in range(4)]
    rows = arrived.reshape(16, 2, CAP, 256).transpose(1, 0, 2, 3).reshape(2, HALF, 256)
    rows = exchange(rows, "c").reshape(1, SLOTS, 256)
    tokens = exchange(jnp.broadcast_to(rows, (4, SLOTS, 256)), ACROSS, GATHER)
    partial = call(
        gate_up_kernel, array(4, SLOTS + EXTRA, 256, dtype=F32), at, tokens, *weights, flops=1600 << 20
    ).astype(jnp.float16)
    products = exchange(partial, ACROSS, REDUCE)
    hidden = call(
        hidden_kernel, array(4, SLOTS, 128), jnp.sum(products.astype(F32), axis=0), flops=8 << 20
    )
    hidden = exchange(hidden, ACROSS, GATHER)
    results = call(down_kernel, array(4, SLOTS, 256), at, hidden, *weights, flops=800 << 20)
    summands = exchange(results, ACROSS, REDUCE)
    reduced = call(reduce_kernel, array(2, HALF, 256), summands, flops=4 << 20)
    reduced = exchange(reduced, "c")
    reduced = reduced.reshape(2, 16, CAP, 256).transpose(1, 0, 2, 3).reshape(16, 2 * CAP, 256)
    reduced, q_heads, kv = tie((reduced, q_heads, kv))
    returned = exchange(reduced, "z")
    kv = call(join_kernel, array(16 * TOK, 128), kv, last)
    other = lax.ppermute(kv, "c", [(0, 1), (1, 0)])
    attended = attend(q_heads, kv, other)
    returned, attended = tie((returned, attended))
    moe_out = call(
        combine_kernel,
        array(TOK, 256),
        ids,
        group_weight.reshape(1, TOK),
        expert_weight.T,
        returned.reshape(SLOTS, 256),
        flops=8 << 20,
    )
    return (attended, moe_out)


def solution(mesh):
    torus = Mesh(mesh.devices.reshape(16, 2, 4, 4), ("z", "c", "y", "x"))

    return jax.shard_map(
        on_device,
        mesh=torus,
        in_specs=(
            P(EP, TP),
            P(EP, TP),
            P(EP, TP),
            P(),
            P(),
            P(EP, TP),
            P(EP, None),
            P(EP),
            P(EP, None),
            P(EP, None, TP),
            P(EP, None, TP),
            P(EP, None, TP),
        ),
        out_specs=(P(EP, TP), P(EP, TP)),
        check_vma=False,
    )
```
